256 devices in a mesh: sp: 32 (over z, x), tp: 8 (over y, core).
Axes of the slice: x: 4, y: 4, z: 8, core: 2. Of those that a mesh axis runs over, the one named last changes fastest.
Arguments:
- latents: bfloat16 [16384, 2048], P(('sp', 'tp')), may hold values from -6 to 6
- context: bfloat16 [512, 2048], P('sp'), may hold values from -6 to 6
- cond: float32 [2048], P('sp'), may hold values from -6 to 6
- ctx_cond: float32 [2048], P('sp'), may hold values from -6 to 6
- mod_weight: float32 [2048, 6144], P('sp', 'tp'), may hold values from -0.125 to 0.125
- query_weight: bfloat16 [2048, 2048], P(None, 'tp'), may hold values from -1 to 1, as said below
- key_matrix: bfloat16 [2048, 1024], P(None, 'tp'), may hold values from -1 to 1, as said below
- value_matrix: bfloat16 [2048, 1024], P(None, 'tp'), may hold values from -0.125 to 0.125
- out_weight: bfloat16 [2048, 2048], P('tp'), may hold values from -0.125 to 0.125
- query_gain: float32 [128], replicated, may hold values from 0.7 to 7
- key_gain: float32 [128], replicated, may hold values from 0.7 to 7
Outputs:
- updated: bfloat16 [16384, 2048], P(('sp', 'tp'))
The draws below stay inside these ranges and needn't reach their ends.
Inputs may be any that keep to these rules, and one draw needn't show every extreme that they name: `query_weight`: entries of order 2048 to the power -1/2. `key_matrix`: entries of order 2048 to the power -1/2.
All inputs are finite; a program needn't handle non-finite values.
Results may differ from the reference program's by a relative error of at most 0.0085.
The reference program's roundings to bfloat16 on the way count: a program that leaves them out, or rounds other values in their place, can miss the bound.
Values may be sent and summed in bfloat16 or wider, within the bound.
No kernel may reach another device: no remote copies, remote signals or barrier semaphores. Data moves between devices by JAX's collectives and lax.ppermute only.
A program may use at most 128 MiB of HBM per device.

```python
import math
import jax
import jax.numpy as jnp
from jax import lax

MODEL_DIM = 2048
HEAD_SIZE = 128
QUERY_HEAD_COUNT = 16
KEY_VALUE_HEADS = 8
GRID_W = 64
CTX = 512
TOKENS = 16384


def paired_weights(key):
    query_base = jax.random.normal(jax.random.fold_in(key, 11), (MODEL_DIM, QUERY_HEAD_COUNT * HEAD_SIZE), jnp.float32) * MODEL_DIM ** (-0.5)
    key_start = jax.random.normal(jax.random.fold_in(key, 12), (MODEL_DIM, KEY_VALUE_HEADS * HEAD_SIZE), jnp.float32) * MODEL_DIM ** (-0.5)
    return (query_base, key_start)


def draw_query_weight(key, part):
    return paired_weights(key)[0].astype(jnp.bfloat16)


def draw_key_matrix(key, part):
    return paired_weights(key)[1].astype(jnp.bfloat16)


def draw_query_gain(key, part):
    return jax.random.uniform(jax.random.fold_in(key, 21), (HEAD_SIZE,), jnp.float32, 0.7, 1.3)


def draw_key_gain(key, part):
    return jax.random.uniform(jax.random.fold_in(key, 22), (HEAD_SIZE,), jnp.float32, 0.7, 1.3)


def shard_levels(rng, dims, shards, smallest, high):
    loudness, own = 1.0, jax.random.fold_in(rng, 6)
    for position, parts in shards:
        draws = jnp.exp(jax.random.uniform(jax.random.fold_in(own, position), (parts,), jnp.float32, smallest / len(shards), high / len(shards)))
        loudness = loudness * jnp.repeat(draws, dims[position] // parts).reshape([-1 if axis == position else 1 for axis in range(len(dims))])
    return loudness


def centred(stream_key, dims, width, most, pieces=(), kind=jnp.bfloat16):
    result = jax.random.normal(stream_key, dims, jnp.float32) * width
    if len(pieces) > 0:
        result = shard_levels(stream_key, dims, pieces, -0.22, 0.18) * result
    return jnp.clip(result, min=-most, max=most).astype(kind)


def setup_inputs(seed: int = 0) -> dict:
    key_of = jax.random.split(jax.random.key(seed), 12)
    latents = centred(key_of[0], (TOKENS, MODEL_DIM), 1.0, 6.0, ((0, 256),))
    context = centred(key_of[1], (CTX, MODEL_DIM), 1.0, 6.0, ((0, 32),))
    cond = centred(key_of[2], (MODEL_DIM,), 1.0, 6.0, ((0, 32),), jnp.float32)
    ctx_cond = centred(key_of[3], (MODEL_DIM,), 1.0, 6.0, ((0, 32),), jnp.float32)
    mod_weight = centred(key_of[4], (MODEL_DIM, 3 * MODEL_DIM), MODEL_DIM ** -0.5, 0.125, ((0, 32), (1, 8)), jnp.float32)
    query_weight = draw_query_weight(jax.random.fold_in(key_of[11], 71), 0)
    key_matrix = draw_key_matrix(jax.random.fold_in(key_of[11], 71), 0)
    value_matrix = centred(key_of[7], (MODEL_DIM, KEY_VALUE_HEADS * HEAD_SIZE), MODEL_DIM ** -0.5, 0.125, ((1, 8),))
    out_weight = centred(key_of[8], (QUERY_HEAD_COUNT * HEAD_SIZE, MODEL_DIM), (QUERY_HEAD_COUNT * HEAD_SIZE) ** -0.5, 0.125, ((0, 8),))
    query_gain = draw_query_gain(jax.random.fold_in(key_of[11], 71), 0)
    key_gain = draw_key_gain(jax.random.fold_in(key_of[11], 71), 0)
    return {"latents": latents, "context": context, "cond": cond, "ctx_cond": ctx_cond, "mod_weight": mod_weight, "query_weight": query_weight, "key_matrix": key_matrix, "value_matrix": value_matrix, "out_weight": out_weight, "query_gain": query_gain, "key_gain": key_gain}


NORM_EPS = 1e-06
ROPE_BASE = 10000.0

def normalize(latent_value_rows):
    return latent_value_rows * lax.rsqrt(lax.optimization_barrier(jnp.mean(latent_value_rows * latent_value_rows, axis=-1, keepdims=True)) + NORM_EPS)

def rotate(latent_value_rows, positions):
    quarter = latent_value_rows.shape[-1] // 2
    inv_freq = ROPE_BASE ** (-jnp.arange(quarter, dtype=jnp.float32) / quarter)
    angles = positions.astype(jnp.float32)[:, None] * inv_freq[None, :]
    cos_table = jnp.cos(angles)[:, None, :]
    sin_table = jnp.sin(angles)[:, None, :]
    first, second = (latent_value_rows[..., :quarter], latent_value_rows[..., quarter:])
    return jnp.concatenate([first * cos_table - second * sin_table, second * cos_table + first * sin_table], axis=-1)

def axial(latent_value_rows, positions):
    half_dim = latent_value_rows.shape[-1] // 2
    return jnp.concatenate([rotate(latent_value_rows[..., :half_dim], positions // GRID_W), rotate(latent_value_rows[..., half_dim:], positions % GRID_W)], axis=-1)

def modulate(latent_value_rows, mod_row):
    model_width = latent_value_rows.shape[-1]
    shift_vec = mod_row[:model_width]
    scale_vec = mod_row[model_width:2 * model_width]
    return (normalize(latent_value_rows.astype(jnp.float32)) * (1.0 + scale_vec) + shift_vec).astype(jnp.bfloat16)

def reference(latents, context, cond, ctx_cond, mod_weight, query_weight, key_matrix, value_matrix, out_weight, query_gain, key_gain):
    model_width = latents.shape[1]
    latent_count = latents.shape[0]
    prefix_count = context.shape[0]
    modulation = jnp.dot(jax.nn.silu(jnp.stack([cond, ctx_cond])), mod_weight, precision=lax.Precision.HIGHEST)
    gate_vec = modulation[0, 2 * model_width:]
    normalised_rows = modulate(latents, modulation[0])
    prefix_normalised = modulate(context, modulation[1])
    positions = jnp.arange(latent_count, dtype=jnp.int32)
    query_rows = jnp.dot(normalised_rows, query_weight, preferred_element_type=jnp.float32).reshape(latent_count, QUERY_HEAD_COUNT, HEAD_SIZE)
    query_rows = axial(normalize(query_rows) * query_gain, positions).astype(jnp.bfloat16)
    latent_key_rows = jnp.dot(normalised_rows, key_matrix, preferred_element_type=jnp.float32).reshape(latent_count, KEY_VALUE_HEADS, HEAD_SIZE)
    latent_key_rows = axial(normalize(latent_key_rows) * key_gain, positions).astype(jnp.bfloat16)
    latent_value_rows = jnp.dot(normalised_rows, value_matrix, preferred_element_type=jnp.float32).reshape(latent_count, KEY_VALUE_HEADS, HEAD_SIZE).astype(jnp.bfloat16)
    prefix_keys = jnp.dot(prefix_normalised, key_matrix, preferred_element_type=jnp.float32).reshape(prefix_count, KEY_VALUE_HEADS, HEAD_SIZE)
    prefix_keys = (normalize(prefix_keys) * key_gain).astype(jnp.bfloat16)
    prefix_values = jnp.dot(prefix_normalised, value_matrix, preferred_element_type=jnp.float32).reshape(prefix_count, KEY_VALUE_HEADS, HEAD_SIZE).astype(jnp.bfloat16)
    keys_all = jnp.concatenate([prefix_keys, latent_key_rows], axis=0).astype(jnp.float32)
    values_all = jnp.concatenate([prefix_values, latent_value_rows], axis=0).astype(jnp.float32)
    lift = math.log(latent_count / (2.0 * prefix_count))
    lift_row = jnp.concatenate([jnp.full((prefix_count,), lift, jnp.float32), jnp.zeros((latent_count,), jnp.float32)])
    group_size = QUERY_HEAD_COUNT // KEY_VALUE_HEADS
    rows_per_block = math.gcd(latent_count, 256)
    token_blocks = query_rows.reshape(latent_count // rows_per_block, rows_per_block, KEY_VALUE_HEADS, group_size, HEAD_SIZE)
    inv_root = HEAD_SIZE ** (-0.5)

    def one_block(block):
        scores = jnp.einsum('qhgd,khd->hgqk', block.astype(jnp.float32), keys_all) * inv_root + lift_row
        top_row = lax.optimization_barrier(jnp.max(scores, axis=-1, keepdims=True))
        weights = jnp.exp(scores - top_row)
        total = lax.optimization_barrier(jnp.sum(weights, axis=-1))
        probs = lax.optimization_barrier(weights.astype(jnp.bfloat16)).astype(jnp.float32)
        summed = jnp.einsum('hgqk,khd->qhgd', probs, values_all)
        return (summed / jnp.transpose(total, (2, 0, 1))[..., None]).astype(jnp.bfloat16)
    attended = lax.map(one_block, token_blocks).reshape(latent_count, QUERY_HEAD_COUNT * HEAD_SIZE)
    mixed = jnp.dot(attended, out_weight, preferred_element_type=jnp.float32)
    return (latents.astype(jnp.float32) + gate_vec * normalize(mixed)).astype(jnp.bfloat16)
```

```python
import functools
import math

import jax
import jax.numpy as jnp
import numpy as np
from jax import lax
from jax.experimental import pallas as pl
from jax.experimental.pallas import tpu as pltpu
from jax.sharding import Mesh
from jax.sharding import PartitionSpec as P

GRID_W = 64
SP = ("z", "x")
TP = ("y", "c")
ALL = ("z", "x", "y", "c")
NORM_EPS = 1e-06
ROPE_BASE = 10000.0
HD = 128
OFFS = (0, -1, 1, 2)
BQ = 256

BF = jnp.bfloat16
F32 = jnp.float32


def shift(axis, n, k):
    return [(i, (i + k) % n) for i in range(n)]


def rope_tables(count):
    quarter = HD // 4
    freq = ROPE_BASE ** (-np.arange(quarter, dtype=np.float64) / quarter)

    def pair(n):
        angle = np.arange(n, dtype=np.float64)[:, None] * freq[None, :]
        cos, sin = np.cos(angle), np.sin(angle)
        return np.concatenate([cos, cos], 1), np.concatenate([-sin, sin], 1)

    (rc, rs), (cc, cs) = pair(count // GRID_W), pair(GRID_W)
    left = lambda a: np.concatenate([a, np.zeros_like(a)], 1).astype(np.float32)
    right = lambda a: np.concatenate([np.zeros_like(a), a], 1).astype(np.float32)
    return left(rc), left(rs), right(cc), right(cs)


def rms(v):
    return v * lax.rsqrt(jnp.mean(v * v, axis=-1, keepdims=True) + NORM_EPS)


def project_kernel(
    info, mine, theirs, ctx, mod, wq, wk, wv, qg, kg, row_c, row_s, col_c, col_s, q_out, kv_out
):
    width = mine.shape[1]
    rows = GRID_W

    def modulate(v, r):
        scale = mod[r : r + 1, width : 2 * width]
        return (rms(v.astype(F32)) * (1.0 + scale) + mod[r : r + 1, :width]).astype(BF)

    def turn(v, cos, sin):
        lane = lax.broadcasted_iota(jnp.int32, v.shape, 1)
        other = jnp.where(lane % 64 < 32, pltpu.roll(v, HD - 32, 1), pltpu.roll(v, 32, 1))
        return v * cos + other * sin

    def dot(a, b):
        return jnp.dot(a, b, preferred_element_type=F32)

    for side, ref in enumerate((mine, theirs)):
        normed = modulate(ref[...], 0)
        q = dot(normed, wq[...])
        k = dot(normed, wk[...])
        v = dot(normed, wv[...]).astype(BF)
        k = rms(k) * kg[...]
        q0 = rms(q[:, :HD]) * qg[...]
        q1 = rms(q[:, HD:]) * qg[...]
        for j in range(4):
            at = slice(j * rows, (j + 1) * rows)
            tp = info[side * 4 + j]
            grid_row = info[8] + tp
            cos = row_c[pl.ds(grid_row, 1), :] + col_c[...]
            sin = row_s[pl.ds(grid_row, 1), :] + col_s[...]
            to = pl.ds(pl.multiple_of(tp * rows, rows), rows)
            q_out[0, to, :] = turn(q0[at], cos, sin).astype(BF)
            q_out[1, to, :] = turn(q1[at], cos, sin).astype(BF)
            kv_out[to, :HD] = turn(k[at], cos, sin).astype(BF)
            kv_out[to, HD:] = v[at]
    normed = modulate(ctx[...], 1)
    total = 8 * rows
    kv_out[total:, :HD] = (rms(dot(normed, wk[...])) * kg[...]).astype(BF)
    kv_out[total:, HD:] = dot(normed, wv[...]).astype(BF)


def scores_of(q, keys):
    return lax.dot_general(q, keys, (((1,), (1,)), ((), ())), preferred_element_type=F32)


def attend_kernel(*refs, first, last, pieces, lift):
    refs = list(refs)
    take = lambda n: [refs.pop(0) for _ in range(n)]
    scale = HD**-0.5
    c2 = scale * math.log2(math.e)
    if last:
        (info,) = take(1)
    if first:
        q_parts = take(4)
    else:
        q_all, m_in, l_in, acc_in = take(4)
    kv = take(2 * pieces) if last else take(pieces)
    tails = take(7) if last else []
    if last:
        (out,) = take(1)
    elif first:
        q_all, m_out, l_out, acc_out = take(4)
    else:
        m_out, l_out, acc_out = take(3)
    (k_buf, v_buf) = take(2)
    chunk = 512
    v_buf[:, HD:] = jnp.ones((v_buf.shape[0], HD), BF)
    if last:
        kr, vr = kv
        k_buf[:chunk] = kr[:chunk]
        v_buf[:chunk, :HD] = vr[:chunk]
        k_buf[chunk : chunk + 16] = kr[chunk:]
        v_buf[chunk : chunk + 16, :HD] = vr[chunk:]
        for i, t in enumerate(tails):
            at = slice(chunk + 16 * (i + 1), chunk + 16 * (i + 2))
            k_buf[at] = t[chunk:, :HD]
            v_buf[at, :HD] = t[chunk:, HD:]
    else:
        for i, r in enumerate(kv):
            at = slice(i * chunk, (i + 1) * chunk)
            k_buf[at] = r[:chunk, :HD]
            v_buf[at, :HD] = r[:chunk, HD:]
    if first:
        for j, r in enumerate(q_parts):
            for h in range(2):
                q_all[(2 * j + h) * chunk : (2 * j + h + 1) * chunk] = r[h]

    def softmax_block(at):
        s = scores_of(q_all[at], k_buf[...])
        if last:
            column = lax.broadcasted_iota(jnp.int32, (1, s.shape[1]), 1)
            s = jnp.concatenate([s[:, :chunk], s[:, chunk:] + lift / scale], axis=1)
        top = jnp.max(s, axis=1, keepdims=True)
        if first:
            m_new = jnp.broadcast_to(top, (s.shape[0], HD))
        else:
            m_old = m_in[at]
            m_new = jnp.maximum(m_old, top)
        p = jnp.exp2(s * c2 - m_new[:, :1] * c2).astype(BF)
        pv = jnp.dot(p, v_buf[...], preferred_element_type=F32)
        if first:
            return m_new, pv[:, HD:], pv[:, :HD]
        alpha = jnp.exp2((m_old - m_new) * c2)
        return m_new, l_in[at] * alpha + pv[:, HD:], acc_in[at] * alpha + pv[:, :HD]

    if not last:

        def step(b, carry):
            at = pl.ds(pl.multiple_of(b * BQ, BQ), BQ)
            m_out[at], l_out[at], acc_out[at] = softmax_block(at)
            return carry

        lax.fori_loop(0, 4096 // BQ, step, 0, unroll=2)
        return

    per = BQ // GRID_W
    out[:, GRID_W:, HD:] = jnp.zeros((32, 16, HD), BF)

    def step(b, carry):
        part, sub = b // (chunk // BQ), b % (chunk // BQ)
        found = []
        for h in range(2):
            at = pl.ds(pl.multiple_of((part * 2 + h) * chunk + sub * BQ, BQ), BQ)
            m, l, acc = softmax_block(at)
            found.append(((acc / l).astype(BF), m * c2 + jnp.log2(l)))
        for i in range(per):
            rows = slice(i * GRID_W, (i + 1) * GRID_W)
            block = info[9 + part] * 8 + sub * per + i
            for h in range(2):
                out[block, :GRID_W, h * HD : (h + 1) * HD] = found[h][0][rows]
            lse = jnp.concatenate([found[0][1][rows], found[1][1][rows]], axis=0).T[:16]
            high = lse.astype(BF).astype(F32)
            mid = (lse - high).astype(BF).astype(F32)
            low = lse - high - mid
            line = lax.broadcasted_iota(jnp.int32, lse.shape, 0)
            packed = jnp.where(line == 0, high, jnp.where(line == 1, mid, jnp.where(line == 2, low, 0.0)))
            out[block, GRID_W:, :HD] = packed.astype(BF)
        return carry

    lax.fori_loop(0, 4 * (chunk // BQ), step, 0)


def attend(first, last, pieces, lift, operands):
    rows = 4096
    state = [
        jax.ShapeDtypeStruct((rows, HD), F32),
        jax.ShapeDtypeStruct((rows, HD), F32),
        jax.ShapeDtypeStruct((rows, HD), F32),
    ]
    keys = 640 if last else 512 * pieces
    vmem = pl.BlockSpec(memory_space=pltpu.VMEM)
    specs = [vmem] * len(operands)
    if last:
        specs[0] = pl.BlockSpec(memory_space=pltpu.SMEM)
        shape = [jax.ShapeDtypeStruct((32, GRID_W + 16, 2 * HD), BF)]
        alias = {}
    elif first:
        shape = [jax.ShapeDtypeStruct((rows, HD), BF)] + state
        alias = {}
    else:
        shape = state
        alias = {1: 0, 2: 1, 3: 2}
    return pl.pallas_call(
        functools.partial(attend_kernel, first=first, last=last, pieces=1 if last else pieces, lift=lift),
        out_shape=shape,
        in_specs=specs,
        out_specs=[vmem] * len(shape),
        input_output_aliases=alias,
        scratch_shapes=[pltpu.VMEM((keys, HD), BF), pltpu.VMEM((keys, 2 * HD), BF)],
        compiler_params=pltpu.CompilerParams(vmem_limit_bytes=56 * 2**20),
        cost_estimate=pl.CostEstimate(
            flops=rows * keys * 4 * HD, transcendentals=rows * keys, bytes_accessed=2 * 2**20
        ),
        name="attend_last" if last else ("attend_first" if first else "attend_more"),
    )(*operands)


def finish_kernel(info, got, near, far, near_c, far_c, lat, gate, out, att):
    for j in range(8):
        tp = info[j]
        lse = []
        for x in range(4):
            tail = got[x * 8 + tp, GRID_W:, :HD].astype(F32)
            lse.append(tail[0:1] + tail[1:2] + tail[2:3])
        top = jnp.maximum(jnp.maximum(lse[0], lse[1]), jnp.maximum(lse[2], lse[3]))
        share = [jnp.exp2(v - top) for v in lse]
        inv = 1.0 / (share[0] + share[1] + share[2] + share[3])
        total = None
        for x in range(4):
            w = jnp.broadcast_to(share[x] * inv, (HD, HD)).T
            w = jnp.concatenate([w[:GRID_W], w[GRID_W:]], axis=1)
            term = got[x * 8 + tp, :GRID_W, :].astype(F32) * w
            total = term if total is None else total + term
        att[:, j * 256 : (j + 1) * 256] = total.astype(BF)
    mixed = None
    at = 0
    for ref in (near, far, near_c, far_c):
        n = ref.shape[0]
        part = jnp.dot(att[:, at : at + n], ref[...], preferred_element_type=F32)
        mixed = part if mixed is None else mixed + part
        at += n
    out[...] = (lat[...].astype(F32) + gate[...] * rms(mixed)).astype(BF)


def body(
    latents, context, cond, ctx_cond, mod_weight, query_weight, key_matrix, value_matrix, out_weight,
    query_gain, key_gain,
):
    width = latents.shape[1]
    y, c = lax.axis_index("y"), lax.axis_index("c")
    sp = lax.axis_index(SP)
    tp_mine = jnp.stack([((y + d) % 4) * 2 + c for d in OFFS])
    tp_theirs = jnp.stack([((y + d) % 4) * 2 + 1 - c for d in OFFS])
    x_at = jnp.stack([(lax.axis_index("x") + d) % 4 for d in OFFS])
    info = jnp.concatenate([tp_mine, tp_theirs, (sp * 8)[None], x_at]).astype(jnp.int32)

    def over_four(v, axis):
        return [
            v,
            lax.ppermute(v, axis, shift(axis, 4, 1)),
            lax.ppermute(v, axis, shift(axis, 4, -1)),
            lax.ppermute(v, axis, shift(axis, 4, 2)),
        ]

    swap = [(0, 1), (1, 0)]
    rows4 = over_four(latents, "y")
    partial = jnp.dot(
        jax.nn.silu(jnp.stack([cond, ctx_cond])), mod_weight, precision=lax.Precision.HIGHEST
    )
    shares = lax.all_to_all(jnp.broadcast_to(partial[None], (32,) + partial.shape), SP, 0, 0)
    mine = jnp.concatenate(rows4, axis=0)
    theirs = lax.ppermute(mine, "c", swap)
    summed = jnp.sum(shares, axis=0)
    gathered = lax.all_to_all(jnp.broadcast_to(summed[None], (8,) + summed.shape), TP, 0, 0)
    modulation = gathered.transpose(1, 0, 2).reshape(2, -1)
    count = 16384
    tables = [jnp.asarray(t) for t in rope_tables(count)]
    vmem = pl.BlockSpec(memory_space=pltpu.VMEM)
    q, kv = pl.pallas_call(
        project_kernel,
        out_shape=[
            jax.ShapeDtypeStruct((2, 512, HD), BF),
            jax.ShapeDtypeStruct((528, 2 * HD), BF),
        ],
        in_specs=[pl.BlockSpec(memory_space=pltpu.SMEM)] + [vmem] * 13,
        out_specs=[vmem] * 2,
        compiler_params=pltpu.CompilerParams(vmem_limit_bytes=56 * 2**20),
        cost_estimate=pl.CostEstimate(flops=2 * 528 * 2048 * 512, transcendentals=0, bytes_accessed=4 * 2**20),
        name="project",
    )(
        info, mine, theirs, context, modulation, query_weight, key_matrix, value_matrix,
        query_gain[None], key_gain[None], *tables,
    )
    lift = math.log(count / (2.0 * 512))
    up, down = [kv], [kv]
    q_parts = over_four(q, "x")
    for _ in range(3):
        up.append(lax.ppermute(up[-1], "z", shift("z", 8, 1)))
        down.append(lax.ppermute(down[-1], "z", shift("z", 8, -1)))
    k_last = lax.ppermute(up[3][:, :HD], "z", shift("z", 8, 1))
    v_last = lax.ppermute(down[3][:, HD:], "z", shift("z", 8, -1))
    w_up = lax.ppermute(out_weight, "y", shift("y", 4, 1))
    w_down = lax.ppermute(out_weight, "y", shift("y", 4, -1))
    half = out_weight.shape[0] // 2
    far_a = lax.ppermute(w_up[:half], "y", shift("y", 4, 1))
    far_b = lax.ppermute(w_down[half:], "y", shift("y", 4, -1))
    near = jnp.concatenate([out_weight, w_up, w_down], axis=0)
    far = jnp.concatenate([far_a, far_b], axis=0)
    near_c = lax.ppermute(near, "c", swap)
    far_c = lax.ppermute(far, "c", swap)

    q_all, *state = attend(True, False, 1, lift, [*q_parts, kv])
    for t in range(1, 4):
        state = attend(False, False, 2, lift, [q_all, *state, up[t], down[t]])
    tails = [kv] + up[1:] + down[1:]
    (sent,) = attend(False, True, 1, lift, [info, q_all, *state, k_last, v_last, *tails])
    got = lax.all_to_all(sent, ("x", "y", "c"), 0, 0)
    return pl.pallas_call(
        finish_kernel,
        out_shape=jax.ShapeDtypeStruct(latents.shape, BF),
        in_specs=[pl.BlockSpec(memory_space=pltpu.SMEM)] + [vmem] * 7,
        out_specs=vmem,
        scratch_shapes=[pltpu.VMEM((GRID_W, width), BF)],
        compiler_params=pltpu.CompilerParams(vmem_limit_bytes=56 * 2**20),
        cost_estimate=pl.CostEstimate(flops=2 * 64 * 2048 * 2048, transcendentals=0, bytes_accessed=10 * 2**20),
        name="finish",
    )(info, got, near, far, near_c, far_c, latents, modulation[:1, 2 * width :])


def solution(mesh):
    torus = Mesh(mesh.devices.reshape(8, 4, 4, 2), ALL)
    placed = (
        P(ALL, None), P(SP, None), P(SP), P(SP), P(SP, TP), P(None, TP), P(None, TP), P(None, TP),
        P(TP, None), P(), P(),
    )
    return jax.shard_map(body, mesh=torus, in_specs=placed, out_specs=P(ALL, None), check_vma=False)
```

```python
import functools
import math

import jax
import jax.numpy as jnp
import numpy as np
from jax import lax
from jax.experimental import pallas as pl
from jax.experimental.pallas import tpu as pltpu
from jax.sharding import Mesh
from jax.sharding import PartitionSpec as P

GRID_W = 64
SP = ("z", "x")
TP = ("y", "c")
ALL = ("z", "x", "y", "c")
NORM_EPS = 1e-06
ROPE_BASE = 10000.0
HD = 128
OFFS = (0, -1, 1, 2)
BQ = 512

BF = jnp.bfloat16
F32 = jnp.float32


def shift(n, k):
    return [(i, (i + k) % n) for i in range(n)]


def rope_tables(count):
    quarter = HD // 4
    freq = ROPE_BASE ** (-np.arange(quarter, dtype=np.float64) / quarter)

    def pair(n):
        angle = np.arange(n, dtype=np.float64)[:, None] * freq[None, :]
        cos, sin = np.cos(angle), np.sin(angle)
        return np.concatenate([cos, cos], 1), np.concatenate([-sin, sin], 1)

    (rc, rs), (cc, cs) = pair(count // GRID_W), pair(GRID_W)
    left = lambda a: np.concatenate([a, np.zeros_like(a)], 1).astype(np.float32)
    right = lambda a: np.concatenate([np.zeros_like(a), a], 1).astype(np.float32)
    return left(rc), left(rs), right(cc), right(cs)


def rms(v):
    return v * lax.rsqrt(jnp.mean(v * v, axis=-1, keepdims=True) + NORM_EPS)


def columns_of(mod, row, first, last):
    wide = mod.shape[2]
    found = []
    for piece in range(mod.shape[0]):
        lo, hi = max(first - piece * wide, 0), min(last - piece * wide, wide)
        if lo < hi:
            found.append(mod[piece, row : row + 1, lo:hi])
    return jnp.concatenate(found, axis=1)


def tp_of(offset, core):
    return lax.rem(lax.axis_index("y") + offset + 4, 4) * 2 + core


def project_kernel(*refs):
    blocks, mod, far = list(refs[:7]), refs[7], refs[8:19]
    q_out, kv_out, buf = refs[19:22]
    held, arrived = refs[22:33], refs[33]
    copies = [pltpu.make_async_copy(f, h, arrived.at[i]) for i, (f, h) in enumerate(zip(far, held))]
    for copy in copies:
        copy.start()
    lat, wq, wk, wv, ctx, qg, kg, row_c, row_s, col_c, col_s = held
    blocks.insert(0, lat)
    width = ctx.shape[1]
    rows = GRID_W
    sp = lax.axis_index("z") * 4 + lax.axis_index("x")
    core = lax.axis_index("c")

    def modulate(v, r):
        scale = columns_of(mod, r, width, 2 * width)
        return (rms(v.astype(F32)) * (1.0 + scale) + columns_of(mod, r, 0, width)).astype(BF)

    def turn(v, cos, sin):
        lane = lax.broadcasted_iota(jnp.int32, v.shape, 1)
        other = jnp.where(lane % 64 < 32, pltpu.roll(v, HD - 32, 1), pltpu.roll(v, 32, 1))
        return v * cos + other * sin

    def dot(a, b):
        return jnp.dot(a, b, preferred_element_type=F32)

    for side in range(2):
        for j in (1, 2, 3, 0) if side == 0 else range(4):
            if side == 0 and j == 0:
                for copy in copies:
                    copy.wait()
            buf[j * rows : (j + 1) * rows] = modulate(blocks[side * 4 + j][...], 0)
        normed = buf[...]
        q = dot(normed, wq[...])
        k = dot(normed, wk[...])
        v = dot(normed, wv[...]).astype(BF)
        k = rms(k) * kg[...]
        q0 = rms(q[:, :HD]) * qg[...]
        q1 = rms(q[:, HD:]) * qg[...]
        for j in range(4):
            at = slice(j * rows, (j + 1) * rows)
            tp = tp_of(OFFS[j], core if side == 0 else 1 - core)
            cos = row_c[pl.ds(sp * 8 + tp, 1), :] + col_c[...]
            sin = row_s[pl.ds(sp * 8 + tp, 1), :] + col_s[...]
            to = pl.ds(pl.multiple_of(tp * rows, rows), rows)
            q_out[0, to, :] = turn(q0[at], cos, sin).astype(BF)
            q_out[1, to, :] = turn(q1[at], cos, sin).astype(BF)
            kv_out[to, :HD] = turn(k[at], cos, sin).astype(BF)
            kv_out[to, HD:] = v[at]
    normed = modulate(ctx[...], 1)
    total = 8 * rows
    kv_out[total:, :HD] = (rms(dot(normed, wk[...])) * kg[...]).astype(BF)
    kv_out[total:, HD:] = dot(normed, wv[...]).astype(BF)


def scores_of(q, keys):
    return lax.dot_general(q, keys, (((1,), (1,)), ((), ())), preferred_element_type=F32)


def attend_kernel(*refs, first, last, pieces, lift):
    refs = list(refs)
    take = lambda n: [refs.pop(0) for _ in range(n)]
    scale = HD**-0.5
    c2 = scale * math.log2(math.e)
    if first:
        q_parts = take(4)
    else:
        q_all, m_in, l_in, acc_in = take(4)
    kv = take(2 * pieces) if last else take(pieces)
    tails = take(7) if last else []
    if last:
        (out,) = take(1)
    elif first:
        q_all, m_out, l_out, acc_out = take(4)
    else:
        m_out, l_out, acc_out = take(3)
    (k_buf, v_buf) = take(2)
    chunk = 512
    if last:
        kr, vr = kv
        k_buf[:chunk] = kr[:chunk]
        v_buf[:chunk] = vr[:chunk]
        k_buf[chunk : chunk + 16] = kr[chunk:]
        v_buf[chunk : chunk + 16] = vr[chunk:]
        for i, t in enumerate(tails):
            at = slice(chunk + 16 * (i + 1), chunk + 16 * (i + 2))
            k_buf[at] = t[chunk:, :HD]
            v_buf[at] = t[chunk:, HD:]
    else:
        for i, r in enumerate(kv):
            at = slice(i * chunk, (i + 1) * chunk)
            k_buf[at] = r[:chunk, :HD]
            v_buf[at] = r[:chunk, HD:]
    if first:
        for j, r in enumerate(q_parts):
            for h in range(2):
                q_all[(2 * j + h) * chunk : (2 * j + h + 1) * chunk] = r[h]

    def tree(values, op):
        while len(values) > 1:
            odd = values[len(values) // 2 * 2 :]
            values = [op(values[2 * i], values[2 * i + 1]) for i in range(len(values) // 2)] + odd
        return values[0]

    def softmax_block(at):
        s = scores_of(q_all[at], k_buf[...])
        tiles = [s[:, i * HD : (i + 1) * HD] for i in range(s.shape[1] // HD)]
        if last:
            tiles[-1] = tiles[-1] + lift / scale
        top = jnp.max(tree(tiles, jnp.maximum), axis=1, keepdims=True)
        if first:
            m_new = jnp.broadcast_to(top, (s.shape[0], HD))
        else:
            m_old = m_in[at]
            m_new = jnp.maximum(m_old, top)
        base = m_new * c2
        probs = [jnp.exp2(t * c2 - base) for t in tiles]
        p = jnp.concatenate([t.astype(BF) for t in probs], axis=1)
        pv = jnp.dot(p, v_buf[...], preferred_element_type=F32)
        sums = tree(probs, jnp.add)
        if first:
            return m_new, sums, pv
        alpha = jnp.exp2((m_old - m_new) * c2)
        return m_new, l_in[at] * alpha + sums, acc_in[at] * alpha + pv

    if not last:

        def step(b, carry):
            at = pl.ds(pl.multiple_of(b * BQ, BQ), BQ)
            m_out[at], l_out[at], acc_out[at] = softmax_block(at)
            return carry

        lax.fori_loop(0, 4096 // BQ, step, 0, unroll=2)
        return

    per = BQ // GRID_W
    out[:, GRID_W:, HD:] = jnp.zeros((32, 16, HD), BF)

    def step(b, carry):
        part, sub = b // (chunk // BQ), b % (chunk // BQ)
        x_at = lax.rem(lax.axis_index("x") + jnp.where(part == 1, 3, jnp.where(part == 0, 0, part - 1)), 4)
        found = []
        for h in range(2):
            at = pl.ds(pl.multiple_of((part * 2 + h) * chunk + sub * BQ, BQ), BQ)
            m, l, acc = softmax_block(at)
            l = jnp.broadcast_to(jnp.sum(l, axis=1, keepdims=True), l.shape)
            found.append(((acc / l).astype(BF), m * c2 + jnp.log2(l)))
        for i in range(per):
            rows = slice(i * GRID_W, (i + 1) * GRID_W)
            block = x_at * 8 + sub * per + i
            for h in range(2):
                out[block, :GRID_W, h * HD : (h + 1) * HD] = found[h][0][rows]
            lse = jnp.concatenate([found[0][1][rows], found[1][1][rows]], axis=0).T[:16]
            high = lse.astype(BF).astype(F32)
            mid = (lse - high).astype(BF).astype(F32)
            low = lse - high - mid
            line = lax.broadcasted_iota(jnp.int32, lse.shape, 0)
            packed = jnp.where(line == 0, high, jnp.where(line == 1, mid, jnp.where(line == 2, low, 0.0)))
            out[block, GRID_W:, :HD] = packed.astype(BF)
        return carry

    lax.fori_loop(0, 4 * (chunk // BQ), step, 0)


def near(v):
    return pltpu.with_memory_space_constraint(v, pltpu.VMEM)


VMEM = pl.BlockSpec(memory_space=pltpu.VMEM)


def attend(first, last, pieces, lift, operands):
    rows = 4096
    state = [pltpu.VMEM((rows, HD), F32)] * 3
    keys = 640 if last else 512 * pieces
    alias = {}
    if last:
        shape = [pltpu.VMEM((32, GRID_W + 16, 2 * HD), BF)]
    elif first:
        shape = [pltpu.VMEM((rows, HD), BF)] + state
    else:
        shape = state
        alias = {1: 0, 2: 1, 3: 2}
    return pl.pallas_call(
        functools.partial(attend_kernel, first=first, last=last, pieces=1 if last else pieces, lift=lift),
        out_shape=shape,
        in_specs=[VMEM] * len(operands),
        out_specs=[VMEM] * len(shape),
        input_output_aliases=alias,
        scratch_shapes=[pltpu.VMEM((keys, HD), BF), pltpu.VMEM((keys, HD), BF)],
        compiler_params=pltpu.CompilerParams(vmem_limit_bytes=32 * 2**20),
        cost_estimate=pl.CostEstimate(
            flops=rows * keys * 4 * HD, transcendentals=rows * keys, bytes_accessed=2 * 2**20
        ),
        name="attend_last" if last else ("attend_first" if first else "attend_more"),
    )(*[near(v) for v in operands])


def finish_kernel(got, w0, w1, w2, w3, w4, w5, w6, w7, lat, mod, out, att, held, arrived):
    copies = [
        pltpu.make_async_copy(ref, held.at[j], arrived.at[j])
        for j, ref in enumerate((w0, w1, w2, w3, w4, w5, w6, w7))
    ]
    for copy in copies:
        copy.start()
    core = lax.axis_index("c")
    width = lat.shape[1]
    for j in range(8):
        side, piece = j // 4, j % 4
        owner = core if side == 0 else 1 - core
        ahead = 1 - 2 * owner
        tp = tp_of((0, -ahead, ahead, 2)[piece], owner)
        lse = []
        for x in range(4):
            tail = got[x * 8 + tp, GRID_W:, :HD].astype(F32)
            lse.append(tail[0:1] + tail[1:2] + tail[2:3])
        top = jnp.maximum(jnp.maximum(lse[0], lse[1]), jnp.maximum(lse[2], lse[3]))
        share = [jnp.exp2(v - top) for v in lse]
        inv = 1.0 / (share[0] + share[1] + share[2] + share[3])
        total = None
        for x in range(4):
            w = jnp.broadcast_to(share[x] * inv, (HD, HD)).T
            w = jnp.concatenate([w[:GRID_W], w[GRID_W:]], axis=1)
            term = got[x * 8 + tp, :GRID_W, :].astype(F32) * w
            total = term if total is None else total + term
        att[:, j * 256 : (j + 1) * 256] = total.astype(BF)
    mixed = None
    for j, copy in enumerate(copies):
        copy.wait()
        part = jnp.dot(att[:, j * 256 : (j + 1) * 256], held[j], preferred_element_type=F32)
        mixed = part if mixed is None else mixed + part
    gate = columns_of(mod, 0, 2 * width, 3 * width)
    out[...] = (lat[...].astype(F32) + gate * rms(mixed)).astype(BF)


def body(
    latents, context, cond, ctx_cond, mod_weight, query_weight, key_matrix, value_matrix, out_weight,
    query_gain, key_gain,
):
    def over_four(v, axis):
        return [
            v,
            lax.ppermute(v, axis, shift(4, 1)),
            lax.ppermute(v, axis, shift(4, -1)),
            lax.ppermute(v, axis, shift(4, 2)),
        ]

    def swap(v):
        return lax.ppermute(v, "c", [(0, 1), (1, 0)])

    ahead = [(2 * i + c, 2 * ((i + 1 - 2 * c) % 4) + c) for i in range(4) for c in range(2)]
    behind = [(b, a) for a, b in ahead]

    mine = over_four(latents, "y")
    partial = jnp.dot(
        jax.nn.silu(jnp.stack([cond, ctx_cond])), mod_weight, precision=lax.Precision.HIGHEST
    )
    shares = lax.all_to_all(jnp.broadcast_to(partial[None], (32,) + partial.shape), SP, 0, 0)
    theirs = [swap(v) for v in mine]
    summed = jnp.sum(shares, axis=0)
    modulation = lax.all_to_all(jnp.broadcast_to(summed[None], (8,) + summed.shape), TP, 0, 0)
    count = 16384
    tables = [jnp.asarray(t) for t in rope_tables(count)]
    loaded = [
        latents, query_weight, key_matrix, value_matrix, context, query_gain[None], key_gain[None], *tables,
    ]
    q, kv = pl.pallas_call(
        project_kernel,
        out_shape=[pltpu.VMEM((2, 512, HD), BF), pltpu.VMEM((528, 2 * HD), BF)],
        in_specs=[VMEM] * 8 + [pl.BlockSpec(memory_space=pltpu.HBM)] * len(loaded),
        out_specs=[VMEM] * 2,
        scratch_shapes=[pltpu.VMEM((256, 2048), BF)]
        + [pltpu.VMEM(v.shape, v.dtype) for v in loaded]
        + [pltpu.SemaphoreType.DMA((len(loaded),))],
        compiler_params=pltpu.CompilerParams(vmem_limit_bytes=32 * 2**20),
        cost_estimate=pl.CostEstimate(flops=2 * 528 * 2048 * 512, transcendentals=0, bytes_accessed=4 * 2**20),
        name="project",
    )(
        *[near(v) for v in mine[1:] + theirs],
        near(modulation),
        *[pltpu.with_memory_space_constraint(v, pltpu.HBM) for v in loaded],
    )
    lift = math.log(count / (2.0 * 512))
    kv, late_weight = lax.optimization_barrier((kv, out_weight))
    up, down = [kv], [kv]
    up.append(lax.ppermute(kv, "z", shift(8, 1)))
    down.append(lax.ppermute(kv, "z", shift(8, -1)))
    q_parts = over_four(q, "x")
    for _ in range(2):
        up.append(lax.ppermute(up[-1], "z", shift(8, 1)))
        down.append(lax.ppermute(down[-1], "z", shift(8, -1)))
    k_last = lax.ppermute(up[3][:, :HD], "z", shift(8, 1))
    v_last = lax.ppermute(down[3][:, HD:], "z", shift(8, -1))
    first = lax.ppermute(late_weight, TP, ahead)
    second = lax.ppermute(late_weight, TP, behind)
    weights = [out_weight, first, second, lax.ppermute(first, TP, ahead)]
    weights += [swap(late_weight), swap(first), swap(second)]
    weights.append(swap(weights[3]))

    q_all, *state = attend(True, False, 1, lift, [*q_parts, kv])
    for t in range(1, 4):
        state = attend(False, False, 2, lift, [q_all, *state, up[t], down[t]])
    tails = [kv] + up[1:] + down[1:]
    (sent,) = attend(False, True, 1, lift, [q_all, *state, k_last, v_last, *tails])
    got = lax.all_to_all(sent, ("x", "y", "c"), 0, 0)
    return pl.pallas_call(
        finish_kernel,
        out_shape=jax.ShapeDtypeStruct(latents.shape, BF),
        in_specs=[VMEM] + [pl.BlockSpec(memory_space=pltpu.HBM)] * 8 + [VMEM] * 2,
        out_specs=VMEM,
        scratch_shapes=[
            pltpu.VMEM(latents.shape, BF),
            pltpu.VMEM((8,) + out_weight.shape, BF),
            pltpu.SemaphoreType.DMA((8,)),
        ],
        compiler_params=pltpu.CompilerParams(vmem_limit_bytes=32 * 2**20),
        cost_estimate=pl.CostEstimate(flops=2 * 64 * 2048 * 2048, transcendentals=0, bytes_accessed=10 * 2**20),
        name="finish",
    )(
        near(got),
        *[pltpu.with_memory_space_constraint(v, pltpu.HBM) for v in weights],
        near(latents),
        near(modulation),
    )


def solution(mesh):
    torus = Mesh(mesh.devices.reshape(8, 4, 4, 2), ALL)
    placed = (
        P(ALL, None), P(SP, None), P(SP), P(SP), P(SP, TP), P(None, TP), P(None, TP), P(None, TP),
        P(TP, None), P(), P(),
    )

    return jax.shard_map(body, mesh=torus, in_specs=placed, out_specs=P(ALL, None), check_vma=False)
```

```python
import functools
import math

import jax
import jax.numpy as jnp
import numpy as np
from jax import lax
from jax.experimental import pallas as pl
from jax.experimental.pallas import tpu as pltpu
from jax.sharding import Mesh
from jax.sharding import PartitionSpec as P

GRID_W = 64
SP = ("z", "x")
TP = ("y", "c")
ALL = ("z", "x", "y", "c")
NORM_EPS = 1e-06
ROPE_BASE = 10000.0
HD = 128
OFFS = (0, -1, 1, 2)

BF = jnp.bfloat16
F32 = jnp.float32


def shift(n, k):
    return [(i, (i + k) % n) for i in range(n)]


def rope_tables(count):
    quarter = HD // 4
    freq = ROPE_BASE ** (-np.arange(quarter, dtype=np.float64) / quarter)

    def table(positions, right):
        angle = np.asarray(positions, np.float64)[:, None] * freq[None, :]
        cos, sin = np.cos(angle), np.sin(angle)
        both = np.stack([np.concatenate([cos, cos], 1), np.concatenate([-sin, sin], 1)])
        blank = np.zeros_like(both)
        return np.concatenate([blank, both] if right else [both, blank], 2).astype(np.float32)

    rows = count // GRID_W
    return table(range(0, rows, 8), False), table(range(8), False), table(range(GRID_W), True)


def rms(v):
    return v * lax.rsqrt(jnp.mean(v * v, axis=-1, keepdims=True) + NORM_EPS)


def columns_of(mod, row, first, last):
    wide = mod.shape[2]
    found = []
    for piece in range(mod.shape[0]):
        lo, hi = max(first - piece * wide, 0), min(last - piece * wide, wide)
        if lo < hi:
            found.append(mod[piece, row : row + 1, lo:hi])
    return jnp.concatenate(found, axis=1)


def tp_of(offset, core):
    return lax.rem(lax.axis_index("y") + offset + 4, 4) * 2 + core


def project_kernel(*refs):
    blocks, mod, far = list(refs[:7]), refs[7], refs[8:18]
    q_out, kv_out, buf = refs[18:21]
    held, arrived = refs[21:31], refs[31]
    copies = [pltpu.make_async_copy(f, h, arrived.at[i]) for i, (f, h) in enumerate(zip(far, held))]
    for copy in copies:
        copy.start()
    lat, wq, wk, wv, ctx, qg, kg, eights, ones, cols = held
    blocks.insert(0, lat)
    width = ctx.shape[1]
    rows = GRID_W
    sp = lax.axis_index("z") * 4 + lax.axis_index("x")
    core = lax.axis_index("c")

    def modulate(v, r):
        scale = columns_of(mod, r, width, 2 * width)
        return (rms(v.astype(F32)) * (1.0 + scale) + columns_of(mod, r, 0, width)).astype(BF)

    def turn(v, cos, sin):
        lane = lax.broadcasted_iota(jnp.int32, v.shape, 1)
        other = jnp.where(lane % 64 < 32, pltpu.roll(v, HD - 32, 1), pltpu.roll(v, 32, 1))
        return v * cos + other * sin

    def dot(a, b):
        return jnp.dot(a, b, preferred_element_type=F32)

    for side in range(2):
        for j in (1, 2, 3, 0) if side == 0 else range(4):
            if side == 0 and j == 0:
                for copy in copies:
                    copy.wait()
            buf[j * rows : (j + 1) * rows] = modulate(blocks[side * 4 + j][...], 0)
        normed = buf[...]
        q = dot(normed, wq[...])
        k = dot(normed, wk[...])
        v = dot(normed, wv[...]).astype(BF)
        k = rms(k) * kg[...]
        q0 = rms(q[:, :HD]) * qg[...]
        q1 = rms(q[:, HD:]) * qg[...]
        for j in range(4):
            at = slice(j * rows, (j + 1) * rows)
            tp = tp_of(OFFS[j], core if side == 0 else 1 - core)
            c8, s8, c1, s1 = (t[i, pl.ds(p, 1), :] for t, p in ((eights, sp), (ones, tp)) for i in (0, 1))
            cos = c8 * c1 - s8 * s1 + cols[0]
            sin = s8 * c1 + c8 * s1 + cols[1]
            to = pl.ds(pl.multiple_of(tp * rows, rows), rows)
            q_out[0, to, :] = turn(q0[at], cos, sin).astype(BF)
            q_out[1, to, :] = turn(q1[at], cos, sin).astype(BF)
            kv_out[to, :HD] = turn(k[at], cos, sin).astype(BF)
            kv_out[to, HD:] = v[at]
    normed = modulate(ctx[...], 1)
    total = 8 * rows
    kv_out[total:, :HD] = (rms(dot(normed, wk[...])) * kg[...]).astype(BF)
    kv_out[total:, HD:] = dot(normed, wv[...]).astype(BF)


def scores_of(q, keys):
    return lax.dot_general(q, keys, (((1,), (1,)), ((), ())), preferred_element_type=F32)


def tree(values, op):
    while len(values) > 1:
        odd = values[len(values) // 2 * 2 :]
        values = [op(values[2 * i], values[2 * i + 1]) for i in range(len(values) // 2)] + odd
    return values[0]


SCALE = HD**-0.5
C2 = SCALE * math.log2(math.e)
CHUNK = 512


def fill(k_buf, v_buf, pieces):
    for i, r in enumerate(pieces):
        at = slice(i * CHUNK, (i + 1) * CHUNK)
        k_buf[at] = r[:CHUNK, :HD]
        v_buf[at] = r[:CHUNK, HD:]


def softmax_block(q, k_buf, v_buf, before, lift=None):
    s = scores_of(q, k_buf[...])
    tiles = [s[:, i * HD : (i + 1) * HD] for i in range(s.shape[1] // HD)]
    if lift is not None:
        tiles[-1] = tiles[-1] + lift / SCALE
    top = jnp.max(tree(tiles, jnp.maximum), axis=1, keepdims=True)
    if before is None:
        m_new = jnp.broadcast_to(top, (s.shape[0], HD))
    else:
        m_old, l_old, acc_old = before
        m_new = jnp.maximum(m_old, top)
    base = m_new * C2
    probs = [jnp.exp2(t * C2 - base) for t in tiles]
    p = jnp.concatenate([t.astype(BF) for t in probs], axis=1)
    pv = jnp.dot(p, v_buf[...], preferred_element_type=F32)
    sums = tree(probs, jnp.add)
    if before is None:
        return m_new, sums, pv
    alpha = jnp.exp2((m_old - m_new) * C2)
    return m_new, l_old * alpha + sums, acc_old * alpha + pv


def rows_at(b, size=CHUNK):
    return pl.ds(pl.multiple_of(b * size, size), size)


def own_kernel(q, kv, up, down, m, l, acc, k_buf, v_buf):
    fill(k_buf, v_buf, (kv, up, down))

    def step(b, carry):
        at, size = rows_at(b, CHUNK // 2), CHUNK // 2
        m[at], l[at], acc[at] = softmax_block(q[b // 2, rows_at(lax.rem(b, 2), size)], k_buf, v_buf, None)
        return carry

    lax.fori_loop(0, 4, step, 0)


def rest_kernel(q0, q1, q2, q3, m_own, l_own, acc_own, kv, up, down, q_all, m, l, acc, k_buf, v_buf):
    fill(k_buf, v_buf, (kv, up, down))
    for j, r in enumerate((q0, q1, q2, q3)):
        for h in range(2):
            q_all[(2 * j + h) * CHUNK : (2 * j + h + 1) * CHUNK] = r[h]
    for whole, own in ((m, m_own), (l, l_own), (acc, acc_own)):
        whole[: 2 * CHUNK] = own[...]

    def step(b, carry):
        at = rows_at(b)
        m[at], l[at], acc[at] = softmax_block(q_all[at], k_buf, v_buf, None)
        return carry

    lax.fori_loop(2, 8, step, 0)


def more_kernel(q_all, m_in, l_in, acc_in, up, down, m, l, acc, k_buf, v_buf):
    fill(k_buf, v_buf, (up, down))

    def step(b, carry):
        at = rows_at(b)
        m[at], l[at], acc[at] = softmax_block(q_all[at], k_buf, v_buf, (m_in[at], l_in[at], acc_in[at]))
        return carry

    lax.fori_loop(0, 8, step, 0)


def final_kernel(*refs, parts, lift, size):
    q_all, m_in, l_in, acc_in, up, down, k_far, v_far = refs[:8]
    tails = refs[8:15]
    outs, (k_buf, v_buf) = refs[15:-2], refs[-2:]
    fill(k_buf, v_buf, (up, down))
    at = 2 * CHUNK
    k_buf[at : at + CHUNK] = k_far[:CHUNK]
    v_buf[at : at + CHUNK] = v_far[:CHUNK]
    at += CHUNK
    k_buf[at : at + 16] = k_far[CHUNK:]
    v_buf[at : at + 16] = v_far[CHUNK:]
    for t in tails:
        at += 16
        k_buf[at : at + 16] = t[CHUNK:, :HD]
        v_buf[at : at + 16] = t[CHUNK:, HD:]

    subs = CHUNK // size

    def step(b, carry):
        at = rows_at(parts[0] * 2 * subs + b, size)
        sub, h = lax.rem(b, subs), lax.rem(b // subs, 2)
        m, l, acc = softmax_block(q_all[at], k_buf, v_buf, (m_in[at], l_in[at], acc_in[at]), lift)
        l = jnp.broadcast_to(jnp.sum(l, axis=1, keepdims=True), l.shape)
        values = (acc / l).astype(BF)
        lse = m * C2 + jnp.log2(l)
        packed = jnp.zeros((16, HD), F32)
        line = lax.broadcasted_iota(jnp.int32, (16, HD), 0)
        for t in range(size // HD):
            whole = lse[t * HD : (t + 1) * HD].T[:16]
            high = whole.astype(BF).astype(F32)
            mid = (whole - high).astype(BF).astype(F32)
            for i, v in enumerate((high, mid, whole - high - mid)):
                packed = jnp.where(line == 3 * (t + sub * (size // HD)) + i, v, packed)
        for i, out in enumerate(outs):

            @pl.when(b // (2 * subs) == i)
            def _(out=out):
                out[h, rows_at(sub, size)] = values
                rest = out[h, CHUNK:].astype(F32)
                out[h, CHUNK:] = jnp.where(
                    line < 3 * sub * (size // HD), rest, packed
                ).astype(BF)

        return carry

    lax.fori_loop(0, 2 * subs * len(parts), step, 0)


def merge_kernel(p0, p1, p2, p3, out):
    per = HD // GRID_W
    for h in range(2):
        tails = [p[h, CHUNK:].astype(F32) for p in (p0, p1, p2, p3)]
        for t in range(CHUNK // HD):
            lse = [v[3 * t : 3 * t + 1] + v[3 * t + 1 : 3 * t + 2] + v[3 * t + 2 : 3 * t + 3] for v in tails]
            top = tree(lse, jnp.maximum)
            share = [jnp.exp2(v - top) for v in lse]
            inv = 1.0 / tree(share, jnp.add)
            total = None
            for p, v in zip((p0, p1, p2, p3), share):
                w = jnp.broadcast_to(v * inv, (HD, HD)).T
                term = p[h, t * HD : (t + 1) * HD].astype(F32) * w
                total = term if total is None else total + term
            total = total.astype(BF)
            for i in range(per):
                out[t * per + i, :, h * HD : (h + 1) * HD] = total[i * GRID_W : (i + 1) * GRID_W]


def near(v):
    return pltpu.with_memory_space_constraint(v, pltpu.VMEM)


VMEM = pl.BlockSpec(memory_space=pltpu.VMEM)


def call(kernel, operands, shape, keys, rows, alias=None):
    scratch = [pltpu.VMEM((keys, HD), BF)] * 2 if keys else []
    return pl.pallas_call(
        kernel,
        out_shape=shape,
        in_specs=[VMEM] * len(operands),
        out_specs=[VMEM] * len(shape),
        input_output_aliases=alias or {},
        scratch_shapes=scratch,
        compiler_params=pltpu.CompilerParams(vmem_limit_bytes=20 * 2**20),
        cost_estimate=pl.CostEstimate(
            flops=rows * max(keys, 128) * 4 * HD, transcendentals=rows * keys, bytes_accessed=2**20
        ),
    )(*[near(v) for v in operands])


def finish_kernel(got, w0, w1, w2, w3, w4, w5, w6, w7, lat, mod, out):
    core = lax.axis_index("c")
    width = lat.shape[1]
    mixed = None
    for j, weight in enumerate((w0, w1, w2, w3, w4, w5, w6, w7)):
        side, piece = j // 4, j % 4
        owner = core if side == 0 else 1 - core
        ahead = 1 - 2 * owner
        tp = tp_of((0, -ahead, ahead, 2)[piece], owner)
        part = jnp.dot(got[tp], weight[...], preferred_element_type=F32)
        mixed = part if mixed is None else mixed + part
    gate = columns_of(mod, 0, 2 * width, 3 * width)
    out[...] = (lat[...].astype(F32) + gate * rms(mixed)).astype(BF)


def body(
    latents, context, cond, ctx_cond, mod_weight, query_weight, key_matrix, value_matrix, out_weight,
    query_gain, key_gain,
):
    def over_four(v, axis):
        return [
            v,
            lax.ppermute(v, axis, shift(4, 1)),
            lax.ppermute(v, axis, shift(4, -1)),
            lax.ppermute(v, axis, shift(4, 2)),
        ]

    def swap(v):
        return lax.ppermute(v, "c", [(0, 1), (1, 0)])

    ahead = [(2 * i + c, 2 * ((i + 1 - 2 * c) % 4) + c) for i in range(4) for c in range(2)]
    behind = [(b, a) for a, b in ahead]

    mine = over_four(latents, "y")
    partial = jnp.dot(
        jax.nn.silu(jnp.stack([cond, ctx_cond])), mod_weight, precision=lax.Precision.HIGHEST
    )
    shares = lax.all_to_all(jnp.broadcast_to(partial[None], (32,) + partial.shape), SP, 0, 0)
    theirs = [swap(v) for v in mine]
    summed = jnp.sum(shares, axis=0)
    modulation = lax.all_to_all(jnp.broadcast_to(summed[None], (8,) + summed.shape), TP, 0, 0)
    count = 16384
    tables = [jnp.asarray(t) for t in rope_tables(count)]
    loaded = [
        latents, query_weight, key_matrix, value_matrix, context, query_gain[None], key_gain[None], *tables,
    ]
    q, kv = pl.pallas_call(
        project_kernel,
        out_shape=[pltpu.VMEM((2, 512, HD), BF), pltpu.VMEM((528, 2 * HD), BF)],
        in_specs=[VMEM] * 8 + [pl.BlockSpec(memory_space=pltpu.HBM)] * len(loaded),
        out_specs=[VMEM] * 2,
        scratch_shapes=[pltpu.VMEM((256, 2048), BF)]
        + [pltpu.VMEM(v.shape, v.dtype) for v in loaded]
        + [pltpu.SemaphoreType.DMA((len(loaded),))],
        compiler_params=pltpu.CompilerParams(vmem_limit_bytes=20 * 2**20),
        cost_estimate=pl.CostEstimate(flops=2 * 528 * 2048 * 512, transcendentals=0, bytes_accessed=4 * 2**20),
        name="project",
    )(
        *[near(v) for v in mine[1:] + theirs],
        near(modulation),
        *[pltpu.with_memory_space_constraint(v, pltpu.HBM) for v in loaded],
    )
    lift = math.log(count / (2.0 * 512))
    kv, late_weight = lax.optimization_barrier((kv, out_weight))
    up, down = [kv], [kv]
    up.append(lax.ppermute(kv, "z", shift(8, 1)))
    down.append(lax.ppermute(kv, "z", shift(8, -1)))
    q_parts = over_four(q, "x")
    for _ in range(2):
        up.append(lax.ppermute(up[-1], "z", shift(8, 1)))
        down.append(lax.ppermute(down[-1], "z", shift(8, -1)))
    k_far = lax.ppermute(up[3][:, :HD], "z", shift(8, 1))
    v_far = lax.ppermute(down[3][:, HD:], "z", shift(8, -1))
    first = lax.ppermute(late_weight, TP, ahead)
    second = lax.ppermute(late_weight, TP, behind)
    weights = [out_weight, first, second, lax.ppermute(first, TP, ahead)]
    weights += [swap(late_weight), swap(first), swap(second)]
    weights.append(swap(weights[3]))

    rows = 8 * CHUNK
    state_of = lambda n: [pltpu.VMEM((n, HD), F32)] * 3
    firsts = [kv, up[1], down[1]]
    own = call(own_kernel, [q, *firsts], state_of(2 * CHUNK), 3 * CHUNK, 2 * CHUNK)
    q_all, *state = call(
        rest_kernel, [*q_parts, *own, *firsts], [pltpu.VMEM((rows, HD), BF)] + state_of(rows),
        3 * CHUNK, 6 * CHUNK,
    )
    state = call(
        more_kernel, [q_all, *state, up[2], down[2]], state_of(rows), 2 * CHUNK, rows,
        {1: 0, 2: 1, 3: 2},
    )

    def final(*parts):
        return call(
            functools.partial(final_kernel, parts=parts, lift=lift, size=CHUNK * len(parts) // 2),
            [q_all, *state, up[3], down[3], k_far, v_far, kv, *up[1:], *down[1:]],
            [pltpu.VMEM((2, CHUNK + 16, HD), BF)] * len(parts), 3 * CHUNK + HD, 2 * CHUNK * len(parts),
        )

    (to_far,) = final(3)
    partials = [lax.ppermute(to_far, "x", shift(4, 2))]
    to_down, to_up = final(1, 2)
    partials.append(lax.ppermute(to_down, "x", shift(4, -1)))
    partials.append(lax.ppermute(to_up, "x", shift(4, 1)))
    partials += final(0)
    (sent,) = call(merge_kernel, partials, [jax.ShapeDtypeStruct((8, GRID_W, 2 * HD), BF)], 0, CHUNK)
    got = lax.all_to_all(sent, TP, 0, 0)
    operands = [got, *weights, latents, modulation]
    return pl.pallas_call(
        finish_kernel,
        out_shape=jax.ShapeDtypeStruct(latents.shape, BF),
        in_specs=[VMEM] * len(operands),
        out_specs=VMEM,
        compiler_params=pltpu.CompilerParams(vmem_limit_bytes=20 * 2**20),
        cost_estimate=pl.CostEstimate(flops=2 * 64 * 2048 * 2048, transcendentals=0, bytes_accessed=10 * 2**20),
        name="finish",
    )(*[near(v) for v in operands])


def solution(mesh):
    torus = Mesh(mesh.devices.reshape(8, 4, 4, 2), ALL)
    placed = (
        P(ALL, None), P(SP, None), P(SP), P(SP), P(SP, TP), P(None, TP), P(None, TP), P(None, TP),
        P(TP, None), P(), P(),
    )

    return jax.shard_map(body, mesh=torus, in_specs=placed, out_specs=P(ALL, None), check_vma=False)
```

```python
import functools
import math

import jax
import jax.numpy as jnp
import numpy as np
from jax import lax
from jax.experimental import pallas as pl
from jax.experimental.pallas import tpu as pltpu
from jax.sharding import Mesh
from jax.sharding import PartitionSpec as P

GRID_W = 64
SP = ("z", "x")
TP = ("y", "c")
ALL = ("z", "x", "y", "c")
NORM_EPS = 1e-06
ROPE_BASE = 10000.0
HD = 128
OFFS = (0, -1, 1, 2)

BF = jnp.bfloat16
F32 = jnp.float32


def shift(n, k):
    return [(i, (i + k) % n) for i in range(n)]


def rope_tables(count):
    quarter = HD // 4
    freq = ROPE_BASE ** (-np.arange(quarter, dtype=np.float64) / quarter)

    def table(positions, right):
        angle = np.asarray(positions, np.float64)[:, None] * freq[None, :]
        cos, sin = np.cos(angle), np.sin(angle)
        both = np.stack([np.concatenate([cos, cos], 1), np.concatenate([-sin, sin], 1)])
        blank = np.zeros_like(both)
        return np.concatenate([blank, both] if right else [both, blank], 2).astype(np.float32)

    rows = count // GRID_W
    return table(range(0, rows, 8), False), table(range(8), False), table(range(GRID_W), True)


def rms(v):
    return v * lax.rsqrt(jnp.mean(v * v, axis=-1, keepdims=True) + NORM_EPS)


def columns_of(mod, row, first, last):
    wide = mod.shape[2]
    found = []
    for piece in range(mod.shape[0]):
        lo, hi = max(first - piece * wide, 0), min(last - piece * wide, wide)
        if lo < hi:
            found.append(mod[piece, row : row + 1, lo:hi])
    return jnp.concatenate(found, axis=1)


def tp_of(offset, core):
    return lax.rem(lax.axis_index("y") + offset + 4, 4) * 2 + core


def project_kernel(*refs):
    blocks, mod, far = list(refs[:7]), refs[7], refs[8:18]
    q_out, kv_out, buf = refs[18:21]
    held, arrived = refs[21:31], refs[31]
    copies = [pltpu.make_async_copy(f, h, arrived.at[i]) for i, (f, h) in enumerate(zip(far, held))]
    for copy in copies:
        copy.start()
    lat, wq, wk, wv, ctx, qg, kg, eights, ones, cols = held
    blocks.insert(0, lat)
    width = ctx.shape[1]
    rows = GRID_W
    sp = lax.axis_index("z") * 4 + lax.axis_index("x")
    core = lax.axis_index("c")

    def modulate(v, r):
        scale = columns_of(mod, r, width, 2 * width)
        return (rms(v.astype(F32)) * (1.0 + scale) + columns_of(mod, r, 0, width)).astype(BF)

    def turn(v, cos, sin):
        lane = lax.broadcasted_iota(jnp.int32, v.shape, 1)
        other = jnp.where(lane % 64 < 32, pltpu.roll(v, HD - 32, 1), pltpu.roll(v, 32, 1))
        return v * cos + other * sin

    def dot(a, b):
        return jnp.dot(a, b, preferred_element_type=F32)

    for side in range(2):
        for j in (1, 2, 3, 0) if side == 0 else range(4):
            if side == 0 and j == 0:
                for copy in copies:
                    copy.wait()
            buf[j * rows : (j + 1) * rows] = modulate(blocks[side * 4 + j][...], 0)
        normed = buf[...]
        q = dot(normed, wq[...])
        k = dot(normed, wk[...])
        v = dot(normed, wv[...]).astype(BF)
        k = rms(k) * kg[...]
        q0 = rms(q[:, :HD]) * qg[...]
        q1 = rms(q[:, HD:]) * qg[...]
        for j in range(4):
            at = slice(j * rows, (j + 1) * rows)
            tp = tp_of(OFFS[j], core if side == 0 else 1 - core)
            c8, s8, c1, s1 = (t[i, pl.ds(p, 1), :] for t, p in ((eights, sp), (ones, tp)) for i in (0, 1))
            cos = c8 * c1 - s8 * s1 + cols[0]
            sin = s8 * c1 + c8 * s1 + cols[1]
            to = pl.ds(pl.multiple_of(tp * rows, rows), rows)
            q_out[0, to, :] = turn(q0[at], cos, sin).astype(BF)
            q_out[1, to, :] = turn(q1[at], cos, sin).astype(BF)
            kv_out[to, :HD] = turn(k[at], cos, sin).astype(BF)
            kv_out[to, HD:] = v[at]
    normed = modulate(ctx[...], 1)
    total = 8 * rows
    kv_out[total:, :HD] = (rms(dot(normed, wk[...])) * kg[...]).astype(BF)
    kv_out[total:, HD:] = dot(normed, wv[...]).astype(BF)


def scores_of(q, keys):
    return lax.dot_general(q, keys, (((1,), (1,)), ((), ())), preferred_element_type=F32)


def tree(values, op):
    while len(values) > 1:
        odd = values[len(values) // 2 * 2 :]
        values = [op(values[2 * i], values[2 * i + 1]) for i in range(len(values) // 2)] + odd
    return values[0]


SCALE = HD**-0.5
C2 = SCALE * math.log2(math.e)
CHUNK = 512


def fill(k_buf, v_buf, pieces):
    for i, r in enumerate(pieces):
        at = slice(i * CHUNK, (i + 1) * CHUNK)
        k_buf[at] = r[:CHUNK, :HD]
        v_buf[at] = r[:CHUNK, HD:]


def softmax_block(q, k_buf, v_buf, before, lift=None):
    s = scores_of(q, k_buf[...])
    tiles = [s[:, i * HD : (i + 1) * HD] for i in range(s.shape[1] // HD)]
    if lift is not None:
        tiles = tiles[:-2] + [tiles[-2] + lift / SCALE]
    if before is None:
        blank = jnp.zeros((s.shape[0], HD), F32)
        before = (blank - 1e30, blank, blank)
    m_old, l_old, acc_old = before
    m_new = jnp.maximum(m_old, jnp.max(tree(tiles, jnp.maximum), axis=1, keepdims=True))
    base = m_new * C2
    alpha = jnp.exp2((m_old - m_new) * C2)
    probs = [jnp.exp2(t * C2 - base) for t in tiles]
    p = [t.astype(BF) for t in probs]
    if lift is not None:
        p.append(jnp.zeros((s.shape[0], HD), BF))
    pv = jnp.dot(jnp.concatenate(p, axis=1), v_buf[...], preferred_element_type=F32)
    return m_new, l_old * alpha + tree(probs, jnp.add), acc_old * alpha + pv


def rows_at(b, size=CHUNK):
    return pl.ds(pl.multiple_of(b * size, size), size)


def own_kernel(q, kv, up, down, m, l, acc, k_buf, v_buf):
    fill(k_buf, v_buf, (kv, up, down))

    def step(b, carry):
        at, size = rows_at(b, CHUNK // 2), CHUNK // 2
        m[at], l[at], acc[at] = softmax_block(q[b // 2, rows_at(lax.rem(b, 2), size)], k_buf, v_buf, None)
        return carry

    lax.fori_loop(0, 4, step, 0)


def rest_kernel(q0, q1, q2, q3, m_own, l_own, acc_own, kv, up, down, q_all, m, l, acc, k_buf, v_buf):
    fill(k_buf, v_buf, (kv, up, down))
    for j, r in enumerate((q0, q1, q2, q3)):
        for h in range(2):
            q_all[(2 * j + h) * CHUNK : (2 * j + h + 1) * CHUNK] = r[h]
    for whole, own in ((m, m_own), (l, l_own), (acc, acc_own)):
        whole[: 2 * CHUNK] = own[...]

    def step(b, carry):
        at = rows_at(b)
        m[at], l[at], acc[at] = softmax_block(q_all[at], k_buf, v_buf, None)
        return carry

    lax.fori_loop(2, 8, step, 0)


def more_kernel(q_all, m_in, l_in, acc_in, up, down, m, l, acc, k_buf, v_buf):
    fill(k_buf, v_buf, (up, down))

    def step(b, carry):
        at = rows_at(b)
        m[at], l[at], acc[at] = softmax_block(q_all[at], k_buf, v_buf, (m_in[at], l_in[at], acc_in[at]))
        return carry

    lax.fori_loop(0, 8, step, 0)


def final_kernel(*refs, parts, lift, size):
    q_all, m_in, l_in, acc_in, up, down, k_far, v_far = refs[:8]
    tails = refs[8:15]
    outs, (k_buf, v_buf) = refs[15:-2], refs[-2:]
    fill(k_buf, v_buf, (up, down))
    at = 2 * CHUNK
    k_buf[at : at + CHUNK] = k_far[:CHUNK]
    v_buf[at : at + CHUNK] = v_far[:CHUNK]
    at += CHUNK
    k_buf[at : at + 16] = k_far[CHUNK:]
    v_buf[at : at + 16] = v_far[CHUNK:]
    for t in tails:
        at += 16
        k_buf[at : at + 16] = t[CHUNK:, :HD]
        v_buf[at : at + 16] = t[CHUNK:, HD:]
    at += 16
    k_buf[at:] = jnp.zeros((HD, HD), BF)
    v_buf[at:] = jnp.zeros((HD, HD), BF)

    subs = CHUNK // size

    def step(b, carry):
        at = rows_at(parts[0] * 2 * subs + b, size)
        sub, h = lax.rem(b, subs), lax.rem(b // subs, 2)
        m, l, acc = softmax_block(q_all[at], k_buf, v_buf, (m_in[at], l_in[at], acc_in[at]), lift)
        l = jnp.broadcast_to(jnp.sum(l, axis=1, keepdims=True), l.shape)
        values = (acc / l).astype(BF)
        lse = m * C2 + jnp.log2(l)
        packed = jnp.zeros((16, HD), F32)
        line = lax.broadcasted_iota(jnp.int32, (16, HD), 0)
        for t in range(size // HD):
            whole = lse[t * HD : (t + 1) * HD].T[:16]
            high = whole.astype(BF).astype(F32)
            mid = (whole - high).astype(BF).astype(F32)
            for i, v in enumerate((high, mid, whole - high - mid)):
                packed = jnp.where(line == 3 * (t + sub * (size // HD)) + i, v, packed)
        for i, out in enumerate(outs):

            @pl.when(b // (2 * subs) == i)
            def _(out=out):
                out[h, rows_at(sub, size)] = values
                rest = out[h, CHUNK:].astype(F32)
                out[h, CHUNK:] = jnp.where(
                    line < 3 * sub * (size // HD), rest, packed
                ).astype(BF)

        return carry

    lax.fori_loop(0, 2 * subs * len(parts), step, 0)


def merge_kernel(p0, p1, p2, p3, out):
    per = HD // GRID_W
    for h in range(2):
        tails = [p[h, CHUNK:].astype(F32) for p in (p0, p1, p2, p3)]
        for t in range(CHUNK // HD):
            lse = [v[3 * t : 3 * t + 1] + v[3 * t + 1 : 3 * t + 2] + v[3 * t + 2 : 3 * t + 3] for v in tails]
            top = tree(lse, jnp.maximum)
            share = [jnp.exp2(v - top) for v in lse]
            inv = 1.0 / tree(share, jnp.add)
            total = None
            for p, v in zip((p0, p1, p2, p3), share):
                w = jnp.broadcast_to(v * inv, (HD, HD)).T
                term = p[h, t * HD : (t + 1) * HD].astype(F32) * w
                total = term if total is None else total + term
            total = total.astype(BF)
            for i in range(per):
                out[t * per + i, :, h * HD : (h + 1) * HD] = total[i * GRID_W : (i + 1) * GRID_W]


def near(v):
    return pltpu.with_memory_space_constraint(v, pltpu.VMEM)


VMEM = pl.BlockSpec(memory_space=pltpu.VMEM)


def share_kernel(*refs):
    far, out, held, arrived = refs[:3], refs[3], refs[4:7], refs[7]
    copies = [pltpu.make_async_copy(f, h, arrived.at[i]) for i, (f, h) in enumerate(zip(far, held))]
    for copy in copies:
        copy.start()
    for copy in copies:
        copy.wait()
    both = jnp.concatenate([held[0][...], held[1][...]], axis=0)
    share = jnp.dot(
        jax.nn.silu(both), held[2][...], precision=lax.Precision.HIGHEST, preferred_element_type=F32
    )
    for i in range(out.shape[0]):
        out[i] = share


def call(kernel, operands, shape, keys, rows, alias=None):
    scratch = [pltpu.VMEM((keys, HD), BF)] * 2 if keys else []
    return pl.pallas_call(
        kernel,
        out_shape=shape,
        in_specs=[VMEM] * len(operands),
        out_specs=[VMEM] * len(shape),
        input_output_aliases=alias or {},
        scratch_shapes=scratch,
        compiler_params=pltpu.CompilerParams(vmem_limit_bytes=20 * 2**20),
        cost_estimate=pl.CostEstimate(
            flops=rows * max(keys, 128) * 4 * HD, transcendentals=rows * keys, bytes_accessed=2**20
        ),
    )(*[near(v) for v in operands])


def finish_kernel(got, w0, w1, w2, w3, w4, w5, w6, w7, lat, mod, out):
    core = lax.axis_index("c")
    width = lat.shape[1]
    mixed = None
    for j, weight in enumerate((w0, w1, w2, w3, w4, w5, w6, w7)):
        side, piece = j // 4, j % 4
        owner = core if side == 0 else 1 - core
        ahead = 1 - 2 * owner
        tp = tp_of((0, -ahead, ahead, 2)[piece], owner)
        part = jnp.dot(got[tp], weight[...], preferred_element_type=F32)
        mixed = part if mixed is None else mixed + part
    gate = columns_of(mod, 0, 2 * width, 3 * width)
    out[...] = (lat[...].astype(F32) + gate * rms(mixed)).astype(BF)


def body(
    latents, context, cond, ctx_cond, mod_weight, query_weight, key_matrix, value_matrix, out_weight,
    query_gain, key_gain,
):
    def over_four(v, axis):
        return [
            v,
            lax.ppermute(v, axis, shift(4, 1)),
            lax.ppermute(v, axis, shift(4, -1)),
            lax.ppermute(v, axis, shift(4, 2)),
        ]

    def swap(v):
        return lax.ppermute(v, "c", [(0, 1), (1, 0)])

    ahead = [(2 * i + c, 2 * ((i + 1 - 2 * c) % 4) + c) for i in range(4) for c in range(2)]
    behind = [(b, a) for a, b in ahead]

    mine = over_four(latents, "y")
    loaded = [cond[None], ctx_cond[None], mod_weight]
    shares = pl.pallas_call(
        share_kernel,
        out_shape=jax.ShapeDtypeStruct((32, 2, mod_weight.shape[1]), F32),
        in_specs=[pl.BlockSpec(memory_space=pltpu.HBM)] * 3,
        out_specs=VMEM,
        scratch_shapes=[pltpu.VMEM(v.shape, F32) for v in loaded] + [pltpu.SemaphoreType.DMA((3,))],
        name="share",
    )(*[pltpu.with_memory_space_constraint(v, pltpu.HBM) for v in loaded])
    shares = lax.all_to_all(shares, SP, 0, 0)
    theirs = [swap(v) for v in mine]
    summed = jnp.sum(shares, axis=0)
    modulation = lax.all_to_all(jnp.broadcast_to(summed[None], (8,) + summed.shape), TP, 0, 0)
    count = 16384
    tables = [jnp.asarray(t) for t in rope_tables(count)]
    loaded = [
        latents, query_weight, key_matrix, value_matrix, context, query_gain[None], key_gain[None], *tables,
    ]
    q, kv = pl.pallas_call(
        project_kernel,
        out_shape=[pltpu.VMEM((2, 512, HD), BF), pltpu.VMEM((528, 2 * HD), BF)],
        in_specs=[VMEM] * 8 + [pl.BlockSpec(memory_space=pltpu.HBM)] * len(loaded),
        out_specs=[VMEM] * 2,
        scratch_shapes=[pltpu.VMEM((256, 2048), BF)]
        + [pltpu.VMEM(v.shape, v.dtype) for v in loaded]
        + [pltpu.SemaphoreType.DMA((len(loaded),))],
        compiler_params=pltpu.CompilerParams(vmem_limit_bytes=20 * 2**20),
        cost_estimate=pl.CostEstimate(flops=2 * 528 * 2048 * 512, transcendentals=0, bytes_accessed=4 * 2**20),
        name="project",
    )(
        *[near(v) for v in mine[1:] + theirs],
        near(modulation),
        *[pltpu.with_memory_space_constraint(v, pltpu.HBM) for v in loaded],
    )
    lift = math.log(count / (2.0 * 512))
    up, down = [kv], [kv]
    up.append(lax.ppermute(kv, "z", shift(8, 1)))
    down.append(lax.ppermute(kv, "z", shift(8, -1)))
    q_parts = over_four(q, "x")
    for _ in range(2):
        up.append(lax.ppermute(up[-1], "z", shift(8, 1)))
        down.append(lax.ppermute(down[-1], "z", shift(8, -1)))
    k_far = lax.ppermute(up[3][:, :HD], "z", shift(8, 1))
    v_far = lax.ppermute(down[3][:, HD:], "z", shift(8, -1))
    first = lax.ppermute(out_weight, TP, ahead)
    second = lax.ppermute(out_weight, TP, behind)
    weights = [out_weight, first, second, lax.ppermute(first, TP, ahead)]
    weights += [swap(out_weight), swap(first), swap(second)]
    weights.append(swap(weights[3]))

    rows = 8 * CHUNK
    state_of = lambda n: [pltpu.VMEM((n, HD), F32)] * 3
    firsts = [kv, up[1], down[1]]
    own = call(own_kernel, [q, *firsts], state_of(2 * CHUNK), 3 * CHUNK, 2 * CHUNK)
    q_all, *state = call(
        rest_kernel, [*q_parts, *own, *firsts], [pltpu.VMEM((rows, HD), BF)] + state_of(rows),
        3 * CHUNK, 6 * CHUNK,
    )
    state = call(
        more_kernel, [q_all, *state, up[2], down[2]], state_of(rows), 2 * CHUNK, rows,
        {1: 0, 2: 1, 3: 2},
    )

    def final(*parts):
        return call(
            functools.partial(final_kernel, parts=parts, lift=lift, size=CHUNK),
            [q_all, *state, up[3], down[3], k_far, v_far, kv, *up[1:], *down[1:]],
            [pltpu.VMEM((2, CHUNK + 16, HD), BF)] * len(parts), 3 * CHUNK + 2 * HD, 2 * CHUNK * len(parts),
        )

    (to_far,) = final(3)
    partials = [lax.ppermute(to_far, "x", shift(4, 2))]
    to_down, to_up = final(1, 2)
    partials.append(lax.ppermute(to_down, "x", shift(4, -1)))
    partials.append(lax.ppermute(to_up, "x", shift(4, 1)))
    partials += final(0)
    (sent,) = call(merge_kernel, partials, [jax.ShapeDtypeStruct((8, GRID_W, 2 * HD), BF)], 0, CHUNK)
    got = lax.all_to_all(sent, TP, 0, 0)
    operands = [got, *weights, latents, modulation]
    return pl.pallas_call(
        finish_kernel,
        out_shape=jax.ShapeDtypeStruct(latents.shape, BF),
        in_specs=[VMEM] * len(operands),
        out_specs=VMEM,
        compiler_params=pltpu.CompilerParams(vmem_limit_bytes=20 * 2**20),
        cost_estimate=pl.CostEstimate(flops=2 * 64 * 2048 * 2048, transcendentals=0, bytes_accessed=10 * 2**20),
        name="finish",
    )(*[near(v) for v in operands])


def solution(mesh):
    torus = Mesh(mesh.devices.reshape(8, 4, 4, 2), ALL)
    placed = (
        P(ALL, None), P(SP, None), P(SP), P(SP), P(SP, TP), P(None, TP), P(None, TP), P(None, TP),
        P(TP, None), P(), P(),
    )

    return jax.shard_map(body, mesh=torus, in_specs=placed, out_specs=P(ALL, None), check_vma=False)
```

```python
import functools
import math

import jax
import jax.numpy as jnp
import numpy as np
from jax import lax
from jax.experimental import pallas as pl
from jax.experimental.pallas import tpu as pltpu
from jax.sharding import Mesh
from jax.sharding import PartitionSpec as P

GRID_W = 64
SP = ("z", "x")
TP = ("y", "c")
ALL = ("z", "x", "y", "c")
NORM_EPS = 1e-06
ROPE_BASE = 10000.0
HD = 128
OFFS = (0, -1, 1, 2)

BF = jnp.bfloat16
F32 = jnp.float32


def shift(n, k):
    return [(i, (i + k) % n) for i in range(n)]


def rope_tables(count):
    quarter = HD // 4
    freq = ROPE_BASE ** (-np.arange(quarter, dtype=np.float64) / quarter)

    def table(positions, right):
        angle = np.asarray(positions, np.float64)[:, None] * freq[None, :]
        cos, sin = np.cos(angle), np.sin(angle)
        both = np.stack([np.concatenate([cos, cos], 1), np.concatenate([-sin, sin], 1)])
        blank = np.zeros_like(both)
        return np.concatenate([blank, both] if right else [both, blank], 2).astype(np.float32)

    rows = count // GRID_W
    return table(range(0, rows, 8), False), table(range(8), False), table(range(GRID_W), True)


def rms(v):
    return v * lax.rsqrt(jnp.mean(v * v, axis=-1, keepdims=True) + NORM_EPS)


def columns_of(mod, row, first, last):
    wide = mod.shape[2]
    found = []
    for piece in range(mod.shape[0]):
        lo, hi = max(first - piece * wide, 0), min(last - piece * wide, wide)
        if lo < hi:
            found.append(mod[piece, row : row + 1, lo:hi])
    return jnp.concatenate(found, axis=1)


def tp_of(offset, core):
    return lax.rem(lax.axis_index("y") + offset + 4, 4) * 2 + core


def project_kernel(*refs):
    blocks, mod, far = list(refs[:7]), refs[7], refs[8:18]
    q_out, kv_out, buf = refs[18:21]
    held, arrived = refs[21:31], refs[31]
    copies = [pltpu.make_async_copy(f, h, arrived.at[i]) for i, (f, h) in enumerate(zip(far, held))]
    for copy in copies:
        copy.start()
    lat, wq, wk, wv, ctx, qg, kg, eights, ones, cols = held
    blocks.insert(0, lat)
    width = ctx.shape[1]
    rows = GRID_W
    sp = lax.axis_index("z") * 4 + lax.axis_index("x")
    core = lax.axis_index("c")

    def modulate(v, r):
        scale = columns_of(mod, r, width, 2 * width)
        return (rms(v.astype(F32)) * (1.0 + scale) + columns_of(mod, r, 0, width)).astype(BF)

    def turn(v, cos, sin):
        lane = lax.broadcasted_iota(jnp.int32, v.shape, 1)
        other = jnp.where(lane % 64 < 32, pltpu.roll(v, HD - 32, 1), pltpu.roll(v, 32, 1))
        return v * cos + other * sin

    def dot(a, b):
        return jnp.dot(a, b, preferred_element_type=F32)

    for side in range(2):
        for j in (1, 2, 3, 0) if side == 0 else range(4):
            if side == 0 and j == 0:
                for copy in copies:
                    copy.wait()
            buf[j * rows : (j + 1) * rows] = modulate(blocks[side * 4 + j][...], 0)
        normed = buf[...]
        q = dot(normed, wq[...])
        k = dot(normed, wk[...])
        v = dot(normed, wv[...]).astype(BF)
        k = rms(k) * kg[...]
        q0 = rms(q[:, :HD]) * qg[...]
        q1 = rms(q[:, HD:]) * qg[...]
        for j in range(4):
            at = slice(j * rows, (j + 1) * rows)
            tp = tp_of(OFFS[j], core if side == 0 else 1 - core)
            c8, s8, c1, s1 = (t[i, pl.ds(p, 1), :] for t, p in ((eights, sp), (ones, tp)) for i in (0, 1))
            cos = c8 * c1 - s8 * s1 + cols[0]
            sin = s8 * c1 + c8 * s1 + cols[1]
            to = pl.ds(pl.multiple_of(tp * rows, rows), rows)
            q_out[0, to, :] = turn(q0[at], cos, sin).astype(BF)
            q_out[1, to, :] = turn(q1[at], cos, sin).astype(BF)
            kv_out[to, :HD] = turn(k[at], cos, sin).astype(BF)
            kv_out[to, HD:] = v[at]
    normed = modulate(ctx[...], 1)
    total = 8 * rows
    kv_out[total:, :HD] = (rms(dot(normed, wk[...])) * kg[...]).astype(BF)
    kv_out[total:, HD:] = dot(normed, wv[...]).astype(BF)


def scores_of(q, keys):
    return lax.dot_general(q, keys, (((1,), (1,)), ((), ())), preferred_element_type=F32)


def tree(values, op):
    while len(values) > 1:
        odd = values[len(values) // 2 * 2 :]
        values = [op(values[2 * i], values[2 * i + 1]) for i in range(len(values) // 2)] + odd
    return values[0]


SCALE = HD**-0.5
C2 = SCALE * math.log2(math.e)
CHUNK = 512


def fill(k_buf, v_buf, pieces):
    for i, r in enumerate(pieces):
        at = slice(i * CHUNK, (i + 1) * CHUNK)
        k_buf[at] = r[:CHUNK, :HD]
        v_buf[at] = r[:CHUNK, HD:]


def softmax_block(q, k_buf, v_buf, before, lift=None):
    s = scores_of(q, k_buf[...])
    tiles = [s[:, i * HD : (i + 1) * HD] for i in range(s.shape[1] // HD)]
    if lift is not None:
        tiles = tiles[:-2] + [tiles[-2] + lift / SCALE]
    if before is None:
        blank = jnp.zeros((s.shape[0], HD), F32)
        before = (blank - 1e30, blank, blank)
    m_old, l_old, acc_old = before
    m_new = jnp.maximum(m_old, jnp.max(tree(tiles, jnp.maximum), axis=1, keepdims=True))
    base = m_new * C2
    alpha = jnp.exp2((m_old - m_new) * C2)
    probs = [jnp.exp2(t * C2 - base) for t in tiles]
    p = [t.astype(BF) for t in probs]
    if lift is not None:
        p.append(jnp.zeros((s.shape[0], HD), BF))
    pv = jnp.dot(jnp.concatenate(p, axis=1), v_buf[...], preferred_element_type=F32)
    return m_new, l_old * alpha + tree(probs, jnp.add), acc_old * alpha + pv


def rows_at(b, size=CHUNK):
    return pl.ds(pl.multiple_of(b * size, size), size)


def own_kernel(q, kv, up, down, m, l, acc, k_buf, v_buf):
    fill(k_buf, v_buf, (kv, up, down))

    def step(b, carry):
        at, size = rows_at(b, CHUNK // 2), CHUNK // 2
        m[at], l[at], acc[at] = softmax_block(q[b // 2, rows_at(lax.rem(b, 2), size)], k_buf, v_buf, None)
        return carry

    lax.fori_loop(0, 4, step, 0)


def rest_kernel(q0, q1, q2, q3, m_own, l_own, acc_own, kv, up, down, q_all, m, l, acc, k_buf, v_buf):
    fill(k_buf, v_buf, (kv, up, down))
    for j, r in enumerate((q0, q1, q2, q3)):
        for h in range(2):
            q_all[(2 * j + h) * CHUNK : (2 * j + h + 1) * CHUNK] = r[h]
    for whole, own in ((m, m_own), (l, l_own), (acc, acc_own)):
        whole[: 2 * CHUNK] = own[...]

    def step(b, carry):
        at = rows_at(b)
        m[at], l[at], acc[at] = softmax_block(q_all[at], k_buf, v_buf, None)
        return carry

    lax.fori_loop(2, 8, step, 0)


def more_kernel(q_all, m_in, l_in, acc_in, up, down, m, l, acc, k_buf, v_buf):
    fill(k_buf, v_buf, (up, down))

    def step(b, carry):
        at = rows_at(b)
        m[at], l[at], acc[at] = softmax_block(q_all[at], k_buf, v_buf, (m_in[at], l_in[at], acc_in[at]))
        return carry

    lax.fori_loop(0, 8, step, 0)


def final_kernel(*refs, parts, lift, size):
    q_all, m_in, l_in, acc_in, up, down, k_far, v_far = refs[:8]
    tails = refs[8:15]
    outs, (k_buf, v_buf) = refs[15:-2], refs[-2:]
    fill(k_buf, v_buf, (up, down))
    at = 2 * CHUNK
    k_buf[at : at + CHUNK] = k_far[:CHUNK]
    v_buf[at : at + CHUNK] = v_far[:CHUNK]
    at += CHUNK
    k_buf[at : at + 16] = k_far[CHUNK:]
    v_buf[at : at + 16] = v_far[CHUNK:]
    for t in tails:
        at += 16
        k_buf[at : at + 16] = t[CHUNK:, :HD]
        v_buf[at : at + 16] = t[CHUNK:, HD:]
    at += 16
    k_buf[at:] = jnp.zeros((HD, HD), BF)
    v_buf[at:] = jnp.zeros((HD, HD), BF)

    subs = CHUNK // size

    def step(b, carry):
        at = rows_at(parts[0] * 2 * subs + b, size)
        sub, h = lax.rem(b, subs), lax.rem(b // subs, 2)
        m, l, acc = softmax_block(q_all[at], k_buf, v_buf, (m_in[at], l_in[at], acc_in[at]), lift)
        l = jnp.broadcast_to(jnp.sum(l, axis=1, keepdims=True), l.shape)
        values = (acc / l).astype(BF)
        lse = m * C2 + jnp.log2(l)
        packed = jnp.zeros((16, HD), F32)
        line = lax.broadcasted_iota(jnp.int32, (16, HD), 0)
        for t in range(size // HD):
            whole = lse[t * HD : (t + 1) * HD].T[:16]
            high = whole.astype(BF).astype(F32)
            mid = (whole - high).astype(BF).astype(F32)
            for i, v in enumerate((high, mid, whole - high - mid)):
                packed = jnp.where(line == 3 * (t + sub * (size // HD)) + i, v, packed)
        for i, out in enumerate(outs):

            @pl.when(b // (2 * subs) == i)
            def _(out=out):
                out[h, rows_at(sub, size)] = values
                rest = out[h, CHUNK:].astype(F32)
                out[h, CHUNK:] = jnp.where(
                    line < 3 * sub * (size // HD), rest, packed
                ).astype(BF)

        return carry

    lax.fori_loop(0, 2 * subs * len(parts), step, 0)


def merge_kernel(p0, p1, p2, p3, out):
    per = HD // GRID_W
    for h in range(2):
        tails = [p[h, CHUNK:].astype(F32) for p in (p0, p1, p2, p3)]
        for t in range(CHUNK // HD):
            lse = [v[3 * t : 3 * t + 1] + v[3 * t + 1 : 3 * t + 2] + v[3 * t + 2 : 3 * t + 3] for v in tails]
            top = tree(lse, jnp.maximum)
            share = [jnp.exp2(v - top) for v in lse]
            inv = 1.0 / tree(share, jnp.add)
            total = None
            for p, v in zip((p0, p1, p2, p3), share):
                w = jnp.broadcast_to(v * inv, (HD, HD)).T
                term = p[h, t * HD : (t + 1) * HD].astype(F32) * w
                total = term if total is None else total + term
            total = total.astype(BF)
            for i in range(per):
                out[t * per + i, :, h * HD : (h + 1) * HD] = total[i * GRID_W : (i + 1) * GRID_W]


def near(v):
    return pltpu.with_memory_space_constraint(v, pltpu.VMEM)


VMEM = pl.BlockSpec(memory_space=pltpu.VMEM)


def share_kernel(*refs):
    far, out, held, arrived = refs[:3], refs[3], refs[4:7], refs[7]
    copies = [pltpu.make_async_copy(f, h, arrived.at[i]) for i, (f, h) in enumerate(zip(far, held))]
    for copy in copies:
        copy.start()
    for copy in copies:
        copy.wait()
    both = jnp.concatenate([held[0][...], held[1][...]], axis=0)
    share = jnp.dot(
        jax.nn.silu(both), held[2][...], precision=lax.Precision.HIGHEST, preferred_element_type=F32
    )
    for i in range(out.shape[0]):
        out[i] = share


def call(kernel, operands, shape, keys, rows, alias=None):
    scratch = [pltpu.VMEM((keys, HD), BF)] * 2 if keys else []
    return pl.pallas_call(
        kernel,
        out_shape=shape,
        in_specs=[VMEM] * len(operands),
        out_specs=[VMEM] * len(shape),
        input_output_aliases=alias or {},
        scratch_shapes=scratch,
        compiler_params=pltpu.CompilerParams(vmem_limit_bytes=20 * 2**20),
        cost_estimate=pl.CostEstimate(
            flops=rows * max(keys, 128) * 4 * HD, transcendentals=rows * keys, bytes_accessed=2**20
        ),
    )(*[near(v) for v in operands])


def finish_kernel(got, w0, w1, w2, w3, w4, w5, w6, w7, lat, mod, out):
    core = lax.axis_index("c")
    width = lat.shape[1]
    mixed = None
    for j, weight in enumerate((w0, w1, w2, w3, w4, w5, w6, w7)):
        side, piece = j // 4, j % 4
        owner = core if side == 0 else 1 - core
        ahead = 1 - 2 * owner
        tp = tp_of((0, -ahead, ahead, 2)[piece], owner)
        part = jnp.dot(got[tp], weight[...], preferred_element_type=F32)
        mixed = part if mixed is None else mixed + part
    gate = columns_of(mod, 0, 2 * width, 3 * width)
    out[...] = (lat[...].astype(F32) + gate * rms(mixed)).astype(BF)


def body(
    latents, context, cond, ctx_cond, mod_weight, query_weight, key_matrix, value_matrix, out_weight,
    query_gain, key_gain,
):
    def over_four(v, axis):
        return [
            v,
            lax.ppermute(v, axis, shift(4, 1)),
            lax.ppermute(v, axis, shift(4, -1)),
            lax.ppermute(v, axis, shift(4, 2)),
        ]

    def swap(v):
        return lax.ppermute(v, "c", [(0, 1), (1, 0)])

    ahead = [(2 * i + c, 2 * ((i + 1 - 2 * c) % 4) + c) for i in range(4) for c in range(2)]
    behind = [(b, a) for a, b in ahead]

    mine = over_four(latents, "y")
    loaded = [cond[None], ctx_cond[None], mod_weight]
    shares = pl.pallas_call(
        share_kernel,
        out_shape=jax.ShapeDtypeStruct((32, 2, mod_weight.shape[1]), F32),
        in_specs=[pl.BlockSpec(memory_space=pltpu.HBM)] * 3,
        out_specs=VMEM,
        scratch_shapes=[pltpu.VMEM(v.shape, F32) for v in loaded] + [pltpu.SemaphoreType.DMA((3,))],
        name="share",
    )(*[pltpu.with_memory_space_constraint(v, pltpu.HBM) for v in loaded])
    shares = lax.all_to_all(shares, SP, 0, 0)
    theirs = [swap(v) for v in mine]
    summed = jnp.sum(shares, axis=0)
    modulation = lax.all_to_all(jnp.broadcast_to(summed[None], (8,) + summed.shape), TP, 0, 0)
    count = 16384
    tables = [jnp.asarray(t) for t in rope_tables(count)]
    loaded = [
        latents, query_weight, key_matrix, value_matrix, context, query_gain[None], key_gain[None], *tables,
    ]
    q, kv = pl.pallas_call(
        project_kernel,
        out_shape=[pltpu.VMEM((2, 512, HD), BF), pltpu.VMEM((528, 2 * HD), BF)],
        in_specs=[VMEM] * 8 + [pl.BlockSpec(memory_space=pltpu.HBM)] * len(loaded),
        out_specs=[VMEM] * 2,
        scratch_shapes=[pltpu.VMEM((256, 2048), BF)]
        + [pltpu.VMEM(v.shape, v.dtype) for v in loaded]
        + [pltpu.SemaphoreType.DMA((len(loaded),))],
        compiler_params=pltpu.CompilerParams(vmem_limit_bytes=20 * 2**20),
        cost_estimate=pl.CostEstimate(flops=2 * 528 * 2048 * 512, transcendentals=0, bytes_accessed=4 * 2**20),
        name="project",
    )(
        *[near(v) for v in mine[1:] + theirs],
        near(modulation),
        *[pltpu.with_memory_space_constraint(v, pltpu.HBM) for v in loaded],
    )
    lift = math.log(count / (2.0 * 512))
    up, down = [kv], [kv]
    up.append(lax.ppermute(kv, "z", shift(8, 1)))
    down.append(lax.ppermute(kv, "z", shift(8, -1)))
    q_parts = over_four(q, "x")
    for _ in range(2):
        up.append(lax.ppermute(up[-1], "z", shift(8, 1)))
        down.append(lax.ppermute(down[-1], "z", shift(8, -1)))
    k_far = lax.ppermute(up[3][:, :HD], "z", shift(8, 1))
    v_far = lax.ppermute(down[3][:, HD:], "z", shift(8, -1))
    first = lax.ppermute(out_weight, TP, ahead)
    second = lax.ppermute(out_weight, TP, behind)
    weights = [out_weight, first, second, lax.ppermute(out_weight, "y", shift(4, 2))]
    weights += [swap(v) for v in weights]

    rows = 8 * CHUNK
    state_of = lambda n: [pltpu.VMEM((n, HD), F32)] * 3
    firsts = [kv, up[1], down[1]]
    own = call(own_kernel, [q, *firsts], state_of(2 * CHUNK), 3 * CHUNK, 2 * CHUNK)
    q_all, *state = call(
        rest_kernel, [*q_parts, *own, *firsts], [pltpu.VMEM((rows, HD), BF)] + state_of(rows),
        3 * CHUNK, 6 * CHUNK,
    )
    state = call(
        more_kernel, [q_all, *state, up[2], down[2]], state_of(rows), 2 * CHUNK, rows,
        {1: 0, 2: 1, 3: 2},
    )

    def final(*parts):
        return call(
            functools.partial(final_kernel, parts=parts, lift=lift, size=CHUNK),
            [q_all, *state, up[3], down[3], k_far, v_far, kv, *up[1:], *down[1:]],
            [pltpu.VMEM((2, CHUNK + 16, HD), BF)] * len(parts), 3 * CHUNK + 2 * HD, 2 * CHUNK * len(parts),
        )

    (to_far,) = final(3)
    partials = [lax.ppermute(to_far, "x", shift(4, 2))]
    to_down, to_up = final(1, 2)
    partials.append(lax.ppermute(to_down, "x", shift(4, -1)))
    partials.append(lax.ppermute(to_up, "x", shift(4, 1)))
    partials += final(0)
    (sent,) = call(merge_kernel, partials, [jax.ShapeDtypeStruct((8, GRID_W, 2 * HD), BF)], 0, CHUNK)
    got = lax.all_to_all(sent, TP, 0, 0)
    operands = [got, *weights, latents, modulation]
    return pl.pallas_call(
        finish_kernel,
        out_shape=jax.ShapeDtypeStruct(latents.shape, BF),
        in_specs=[VMEM] * len(operands),
        out_specs=VMEM,
        compiler_params=pltpu.CompilerParams(vmem_limit_bytes=20 * 2**20),
        cost_estimate=pl.CostEstimate(flops=2 * 64 * 2048 * 2048, transcendentals=0, bytes_accessed=10 * 2**20),
        name="finish",
    )(*[near(v) for v in operands])


def solution(mesh):
    torus = Mesh(mesh.devices.reshape(8, 4, 4, 2), ALL)
    placed = (
        P(ALL, None), P(SP, None), P(SP), P(SP), P(SP, TP), P(None, TP), P(None, TP), P(None, TP),
        P(TP, None), P(), P(),
    )

    return jax.shard_map(body, mesh=torus, in_specs=placed, out_specs=P(ALL, None), check_vma=False)
```

```python
import functools
import math

import jax
import jax.numpy as jnp
import numpy as np
from jax import lax
from jax.experimental import pallas as pl
from jax.experimental.pallas import tpu as pltpu
from jax.sharding import Mesh
from jax.sharding import PartitionSpec as P

GRID_W = 64
SP = ("z", "x")
TP = ("y", "c")
ALL = ("z", "x", "y", "c")
NORM_EPS = 1e-06
ROPE_BASE = 10000.0
HD = 128
OFFS = (0, -1, 1, 2)

BF = jnp.bfloat16
F32 = jnp.float32


def shift(n, k):
    return [(i, (i + k) % n) for i in range(n)]


def rope_tables(count):
    quarter = HD // 4
    freq = ROPE_BASE ** (-np.arange(quarter, dtype=np.float64) / quarter)

    def table(positions, right):
        angle = np.asarray(positions, np.float64)[:, None] * freq[None, :]
        cos, sin = np.cos(angle), np.sin(angle)
        both = np.stack([np.concatenate([cos, cos], 1), np.concatenate([-sin, sin], 1)])
        blank = np.zeros_like(both)
        return np.concatenate([blank, both] if right else [both, blank], 2).astype(np.float32)

    rows = count // GRID_W
    return table(range(0, rows, 8), False), table(range(8), False), table(range(GRID_W), True)


def rms(v):
    return v * lax.rsqrt(jnp.mean(v * v, axis=-1, keepdims=True) + NORM_EPS)


def columns_of(mod, row, first, last):
    wide = mod.shape[2]
    found = []
    for piece in range(8):
        lo, hi = max(first - piece * wide, 0), min(last - piece * wide, wide)
        if lo < hi:
            found.append(tree([mod[8 * x + piece, row : row + 1, lo:hi] for x in range(4)], jnp.add))
    return jnp.concatenate(found, axis=1)


def tp_of(offset, core):
    return lax.rem(lax.axis_index("y") + offset + 4, 4) * 2 + core


def project_kernel(*refs):
    blocks, mod, far = list(refs[:7]), refs[7], refs[8:18]
    q_out, kv_out, buf = refs[18:21]
    held, arrived = refs[21:31], refs[31]
    copies = [pltpu.make_async_copy(f, h, arrived.at[i]) for i, (f, h) in enumerate(zip(far, held))]
    for copy in copies:
        copy.start()
    lat, wq, wk, wv, ctx, qg, kg, eights, ones, cols = held
    blocks.insert(0, lat)
    width = ctx.shape[1]
    rows = GRID_W
    sp = lax.axis_index("z") * 4 + lax.axis_index("x")
    core = lax.axis_index("c")

    vectors = [(columns_of(mod, r, width, 2 * width), columns_of(mod, r, 0, width)) for r in range(2)]

    def modulate(v, r):
        scale, offset = vectors[r]
        return (rms(v.astype(F32)) * (1.0 + scale) + offset).astype(BF)

    def turn(v, cos, sin):
        lane = lax.broadcasted_iota(jnp.int32, v.shape, 1)
        other = jnp.where(lane % 64 < 32, pltpu.roll(v, HD - 32, 1), pltpu.roll(v, 32, 1))
        return v * cos + other * sin

    def dot(a, b):
        return jnp.dot(a, b, preferred_element_type=F32)

    for side in range(2):
        for j in (1, 2, 3, 0) if side == 0 else range(4):
            if side == 0 and j == 0:
                for copy in copies:
                    copy.wait()
            buf[j * rows : (j + 1) * rows] = modulate(blocks[side * 4 + j][...], 0)
        normed = buf[...]
        q = dot(normed, wq[...])
        k = dot(normed, wk[...])
        v = dot(normed, wv[...]).astype(BF)
        k = rms(k) * kg[...]
        q0 = rms(q[:, :HD]) * qg[...]
        q1 = rms(q[:, HD:]) * qg[...]
        for j in range(4):
            at = slice(j * rows, (j + 1) * rows)
            tp = tp_of(OFFS[j], core if side == 0 else 1 - core)
            c8, s8, c1, s1 = (t[i, pl.ds(p, 1), :] for t, p in ((eights, sp), (ones, tp)) for i in (0, 1))
            cos = c8 * c1 - s8 * s1 + cols[0]
            sin = s8 * c1 + c8 * s1 + cols[1]
            to = pl.ds(pl.multiple_of(tp * rows, rows), rows)
            q_out[0, to, :] = turn(q0[at], cos, sin).astype(BF)
            q_out[1, to, :] = turn(q1[at], cos, sin).astype(BF)
            kv_out[to, :HD] = turn(k[at], cos, sin).astype(BF)
            kv_out[to, HD:] = v[at]
    normed = modulate(ctx[...], 1)
    total = 8 * rows
    kv_out[total:, :HD] = (rms(dot(normed, wk[...])) * kg[...]).astype(BF)
    kv_out[total:, HD:] = dot(normed, wv[...]).astype(BF)


def scores_of(q, keys):
    return lax.dot_general(q, keys, (((1,), (1,)), ((), ())), preferred_element_type=F32)


def tree(values, op):
    while len(values) > 1:
        odd = values[len(values) // 2 * 2 :]
        values = [op(values[2 * i], values[2 * i + 1]) for i in range(len(values) // 2)] + odd
    return values[0]


SCALE = HD**-0.5
C2 = SCALE * math.log2(math.e)
CHUNK = 512


def fill(k_buf, v_buf, pieces):
    for i, r in enumerate(pieces):
        at = slice(i * CHUNK, (i + 1) * CHUNK)
        k_buf[at] = r[:CHUNK, :HD]
        v_buf[at] = r[:CHUNK, HD:]


def softmax_block(q, k_buf, v_buf, before, lift=None):
    s = scores_of(q, k_buf[...])
    tiles = [s[:, i * HD : (i + 1) * HD] for i in range(s.shape[1] // HD)]
    if lift is not None:
        tiles = tiles[:-2] + [tiles[-2] + lift / SCALE]
    if before is None:
        blank = jnp.zeros((s.shape[0], HD), F32)
        before = (blank - 1e30, blank, blank)
    m_old, l_old, acc_old = before
    m_new = jnp.maximum(m_old, jnp.max(tree(tiles, jnp.maximum), axis=1, keepdims=True))
    base = m_new * C2
    alpha = jnp.exp2((m_old - m_new) * C2)
    probs = [jnp.exp2(t * C2 - base) for t in tiles]
    p = [t.astype(BF) for t in probs]
    if lift is not None:
        p.append(jnp.zeros((s.shape[0], HD), BF))
    pv = jnp.dot(jnp.concatenate(p, axis=1), v_buf[...], preferred_element_type=F32)
    return m_new, l_old * alpha + tree(probs, jnp.add), acc_old * alpha + pv


def rows_at(b, size=CHUNK):
    return pl.ds(pl.multiple_of(b * size, size), size)


def first_kernel(q, *refs):
    pieces, (m, l, acc, k_buf, v_buf) = refs[:-5], refs[-5:]
    fill(k_buf, v_buf, pieces)

    def step(b, carry):
        at, size = rows_at(b, CHUNK // 2), CHUNK // 2
        m[at], l[at], acc[at] = softmax_block(q[b // 2, rows_at(lax.rem(b, 2), size)], k_buf, v_buf, None)
        return carry

    lax.fori_loop(0, 4, step, 0)


def near_kernel(q0, q1, q2, m_own, l_own, acc_own, kv, up, down, q_all, m, l, acc, k_buf, v_buf):
    fill(k_buf, v_buf, (kv, up, down))
    for j, r in enumerate((q0, q1, q2)):
        for h in range(2):
            q_all[(2 * j + h) * CHUNK : (2 * j + h + 1) * CHUNK] = r[h]
    for whole, own in ((m, m_own), (l, l_own), (acc, acc_own)):
        whole[: 2 * CHUNK] = own[...]

    def step(b, carry):
        at = rows_at(b)
        m[at], l[at], acc[at] = softmax_block(q_all[at], k_buf, v_buf, None)
        return carry

    lax.fori_loop(2, 6, step, 0)


def more_kernel(q_all, m_in, l_in, acc_in, up, down, m, l, acc, k_buf, v_buf):
    fill(k_buf, v_buf, (up, down))

    def step(b, carry):
        at = rows_at(b)
        m[at], l[at], acc[at] = softmax_block(q_all[at], k_buf, v_buf, (m_in[at], l_in[at], acc_in[at]))
        return carry

    lax.fori_loop(0, q_all.shape[0] // CHUNK, step, 0)


def final_kernel(*refs, parts, lift, size):
    q_all, m_in, l_in, acc_in, up, down, k_far, v_far = refs[:8]
    tails = refs[8:15]
    outs, (k_buf, v_buf) = refs[15:-2], refs[-2:]
    fill(k_buf, v_buf, (up, down))
    at = 2 * CHUNK
    k_buf[at : at + CHUNK] = k_far[:CHUNK]
    v_buf[at : at + CHUNK] = v_far[:CHUNK]
    at += CHUNK
    k_buf[at : at + 16] = k_far[CHUNK:]
    v_buf[at : at + 16] = v_far[CHUNK:]
    for t in tails:
        at += 16
        k_buf[at : at + 16] = t[CHUNK:, :HD]
        v_buf[at : at + 16] = t[CHUNK:, HD:]
    at += 16
    k_buf[at:] = jnp.zeros((HD, HD), BF)
    v_buf[at:] = jnp.zeros((HD, HD), BF)

    subs = CHUNK // size

    def step(b, carry):
        at = rows_at(parts[0] * 2 * subs + b, size)
        sub, h = lax.rem(b, subs), lax.rem(b // subs, 2)
        m, l, acc = softmax_block(q_all[at], k_buf, v_buf, (m_in[at], l_in[at], acc_in[at]), lift)
        l = jnp.broadcast_to(jnp.sum(l, axis=1, keepdims=True), l.shape)
        values = (acc / l).astype(BF)
        lse = m * C2 + jnp.log2(l)
        packed = jnp.zeros((16, HD), F32)
        line = lax.broadcasted_iota(jnp.int32, (16, HD), 0)
        for t in range(size // HD):
            whole = lse[t * HD : (t + 1) * HD].T[:16]
            high = whole.astype(BF).astype(F32)
            mid = (whole - high).astype(BF).astype(F32)
            for i, v in enumerate((high, mid, whole - high - mid)):
                packed = jnp.where(line == 3 * (t + sub * (size // HD)) + i, v, packed)
        for i, out in enumerate(outs):

            @pl.when(b // (2 * subs) == i)
            def _(out=out):
                out[h, rows_at(sub, size)] = values
                rest = out[h, CHUNK:].astype(F32)
                out[h, CHUNK:] = jnp.where(
                    line < 3 * sub * (size // HD), rest, packed
                ).astype(BF)

        return carry

    lax.fori_loop(0, 2 * subs * len(parts), step, 0)


def merge_kernel(p0, p1, p2, p3, out):
    per = HD // GRID_W
    for h in range(2):
        tails = [p[h, CHUNK:].astype(F32) for p in (p0, p1, p2, p3)]
        for t in range(CHUNK // HD):
            lse = [v[3 * t : 3 * t + 1] + v[3 * t + 1 : 3 * t + 2] + v[3 * t + 2 : 3 * t + 3] for v in tails]
            top = tree(lse, jnp.maximum)
            share = [jnp.exp2(v - top) for v in lse]
            inv = 1.0 / tree(share, jnp.add)
            total = None
            for p, v in zip((p0, p1, p2, p3), share):
                w = jnp.broadcast_to(v * inv, (HD, HD)).T
                term = p[h, t * HD : (t + 1) * HD].astype(F32) * w
                total = term if total is None else total + term
            total = total.astype(BF)
            for i in range(per):
                out[t * per + i, :, h * HD : (h + 1) * HD] = total[i * GRID_W : (i + 1) * GRID_W]


def near(v):
    return pltpu.with_memory_space_constraint(v, pltpu.VMEM)


VMEM = pl.BlockSpec(memory_space=pltpu.VMEM)


def share_kernel(*refs):
    far, out, held, arrived = refs[:3], refs[3], refs[4:7], refs[7]
    copies = [pltpu.make_async_copy(f, h, arrived.at[i]) for i, (f, h) in enumerate(zip(far, held))]
    for copy in copies:
        copy.start()
    for copy in copies:
        copy.wait()
    both = jnp.concatenate([held[0][...], held[1][...]], axis=0)
    share = jnp.dot(
        jax.nn.silu(both), held[2][...], precision=lax.Precision.HIGHEST, preferred_element_type=F32
    )
    for i in range(out.shape[0]):
        out[i] = share


def call(kernel, operands, shape, keys, rows, alias=None):
    scratch = [pltpu.VMEM((keys, HD), BF)] * 2 if keys else []
    return pl.pallas_call(
        kernel,
        out_shape=shape,
        in_specs=[VMEM] * len(operands),
        out_specs=[VMEM] * len(shape),
        input_output_aliases=alias or {},
        scratch_shapes=scratch,
        compiler_params=pltpu.CompilerParams(vmem_limit_bytes=20 * 2**20),
        cost_estimate=pl.CostEstimate(
            flops=rows * max(keys, 128) * 4 * HD, transcendentals=rows * keys, bytes_accessed=2**20
        ),
    )(*[near(v) for v in operands])


def finish_kernel(got, w0, w1, w2, w3, w4, w5, w6, w7, lat, mod, out):
    core = lax.axis_index("c")
    width = lat.shape[1]
    mixed = None
    for j, weight in enumerate((w0, w1, w2, w3, w4, w5, w6, w7)):
        side, piece = j // 4, j % 4
        owner = core if side == 0 else 1 - core
        ahead = 1 - 2 * owner
        tp = tp_of((0, -ahead, ahead, 2)[piece], owner)
        part = jnp.dot(got[tp], weight[...], preferred_element_type=F32)
        mixed = part if mixed is None else mixed + part
    gate = columns_of(mod, 0, 2 * width, 3 * width)
    out[...] = (lat[...].astype(F32) + gate * rms(mixed)).astype(BF)


def body(
    latents, context, cond, ctx_cond, mod_weight, query_weight, key_matrix, value_matrix, out_weight,
    query_gain, key_gain,
):
    def over_four(v, axis):
        return [
            v,
            lax.ppermute(v, axis, shift(4, 1)),
            lax.ppermute(v, axis, shift(4, -1)),
            lax.ppermute(v, axis, shift(4, 2)),
        ]

    def swap(v):
        return lax.ppermute(v, "c", [(0, 1), (1, 0)])

    ahead = [(2 * i + c, 2 * ((i + 1 - 2 * c) % 4) + c) for i in range(4) for c in range(2)]
    behind = [(b, a) for a, b in ahead]

    mine = over_four(latents, "y")
    loaded = [cond[None], ctx_cond[None], mod_weight]
    shares = pl.pallas_call(
        share_kernel,
        out_shape=jax.ShapeDtypeStruct((16, 2, mod_weight.shape[1]), F32),
        in_specs=[pl.BlockSpec(memory_space=pltpu.HBM)] * 3,
        out_specs=VMEM,
        scratch_shapes=[pltpu.VMEM(v.shape, F32) for v in loaded] + [pltpu.SemaphoreType.DMA((3,))],
        name="share",
    )(*[pltpu.with_memory_space_constraint(v, pltpu.HBM) for v in loaded])
    shares = lax.all_to_all(shares, ("z", "c"), 0, 0)
    theirs = [swap(v) for v in mine]
    summed = jnp.sum(shares.reshape((8, 2) + shares.shape[1:]), axis=0)
    pieces = lax.all_to_all(jnp.broadcast_to(summed[None], (16,) + summed.shape), ("x", "y"), 0, 0)
    modulation = pieces.reshape((32,) + shares.shape[1:])
    count = 16384
    tables = [jnp.asarray(t) for t in rope_tables(count)]
    loaded = [
        latents, query_weight, key_matrix, value_matrix, context, query_gain[None], key_gain[None], *tables,
    ]
    q, kv = pl.pallas_call(
        project_kernel,
        out_shape=[pltpu.VMEM((2, 512, HD), BF), pltpu.VMEM((528, 2 * HD), BF)],
        in_specs=[VMEM] * 8 + [pl.BlockSpec(memory_space=pltpu.HBM)] * len(loaded),
        out_specs=[VMEM] * 2,
        scratch_shapes=[pltpu.VMEM((256, 2048), BF)]
        + [pltpu.VMEM(v.shape, v.dtype) for v in loaded]
        + [pltpu.SemaphoreType.DMA((len(loaded),))],
        compiler_params=pltpu.CompilerParams(vmem_limit_bytes=20 * 2**20),
        cost_estimate=pl.CostEstimate(flops=2 * 528 * 2048 * 512, transcendentals=0, bytes_accessed=4 * 2**20),
        name="project",
    )(
        *[near(v) for v in mine[1:] + theirs],
        near(modulation),
        *[pltpu.with_memory_space_constraint(v, pltpu.HBM) for v in loaded],
    )
    lift = math.log(count / (2.0 * 512))
    up, down = [kv], [kv]
    up.append(lax.ppermute(kv, "z", shift(8, 1)))
    down.append(lax.ppermute(kv, "z", shift(8, -1)))
    q_parts = over_four(q, "x")
    for _ in range(2):
        up.append(lax.ppermute(up[-1], "z", shift(8, 1)))
        down.append(lax.ppermute(down[-1], "z", shift(8, -1)))
    k_far = lax.ppermute(up[3][:, :HD], "z", shift(8, 1))
    v_far = lax.ppermute(down[3][:, HD:], "z", shift(8, -1))
    first = lax.ppermute(out_weight, TP, ahead)
    second = lax.ppermute(out_weight, TP, behind)
    weights = [out_weight, first, second, lax.ppermute(out_weight, "y", shift(4, 2))]
    weights += [swap(v) for v in weights]

    state_of = lambda n: [pltpu.VMEM((n, HD), F32)] * 3
    firsts = [kv, up[1], down[1]]
    own = call(first_kernel, [q, *firsts], state_of(2 * CHUNK), 3 * CHUNK, 2 * CHUNK)
    q_all, *state = call(
        near_kernel, [*q_parts[:3], *own, *firsts],
        [pltpu.VMEM((6 * CHUNK, HD), BF)] + state_of(6 * CHUNK), 3 * CHUNK, 4 * CHUNK,
    )
    state = call(
        more_kernel, [q_all, *state, up[2], down[2]], state_of(6 * CHUNK), 2 * CHUNK, 6 * CHUNK,
        {1: 0, 2: 1, 3: 2},
    )
    far = call(first_kernel, [q_parts[3], *firsts, up[2], down[2]], state_of(2 * CHUNK), 5 * CHUNK, 2 * CHUNK)

    def final(whose, size, *parts):
        return call(
            functools.partial(final_kernel, parts=parts, lift=lift, size=size),
            [*whose, up[3], down[3], k_far, v_far, kv, *up[1:], *down[1:]],
            [pltpu.VMEM((2, CHUNK + 16, HD), BF)] * len(parts), 3 * CHUNK + 2 * HD, 2 * CHUNK * len(parts),
        )

    (to_far,) = final([q_parts[3].reshape(2 * CHUNK, HD), *far], CHUNK, 0)
    partials = [lax.ppermute(to_far, "x", shift(4, 2))]
    to_down, to_up = final([q_all, *state], CHUNK, 1, 2)
    partials.append(lax.ppermute(to_down, "x", shift(4, -1)))
    partials.append(lax.ppermute(to_up, "x", shift(4, 1)))
    partials += final([q_all, *state], CHUNK // 2, 0)
    (sent,) = call(merge_kernel, partials, [jax.ShapeDtypeStruct((8, GRID_W, 2 * HD), BF)], 0, CHUNK)
    got = lax.all_to_all(sent, TP, 0, 0)
    operands = [got, *weights, latents, modulation]
    return pl.pallas_call(
        finish_kernel,
        out_shape=jax.ShapeDtypeStruct(latents.shape, BF),
        in_specs=[VMEM] * len(operands),
        out_specs=VMEM,
        compiler_params=pltpu.CompilerParams(vmem_limit_bytes=20 * 2**20),
        cost_estimate=pl.CostEstimate(flops=2 * 64 * 2048 * 2048, transcendentals=0, bytes_accessed=10 * 2**20),
        name="finish",
    )(*[near(v) for v in operands])


def solution(mesh):
    torus = Mesh(mesh.devices.reshape(8, 4, 4, 2), ALL)
    placed = (
        P(ALL, None), P(SP, None), P(SP), P(SP), P(SP, TP), P(None, TP), P(None, TP), P(None, TP),
        P(TP, None), P(), P(),
    )

    return jax.shard_map(body, mesh=torus, in_specs=placed, out_specs=P(ALL, None), check_vma=False)
```

```python
import functools
import math

import jax
import jax.numpy as jnp
import numpy as np
from jax import lax
from jax.experimental import pallas as pl
from jax.experimental.pallas import tpu as pltpu
from jax.sharding import Mesh
from jax.sharding import PartitionSpec as P

GRID_W = 64
SP = ("z", "x")
TP = ("y", "c")
ALL = ("z", "x", "y", "c")
NORM_EPS = 1e-06
ROPE_BASE = 10000.0
HD = 128
OFFS = (0, -1, 1, 2)

BF = jnp.bfloat16
F32 = jnp.float32


def shift(n, k):
    return [(i, (i + k) % n) for i in range(n)]


def rope_tables(count):
    quarter = HD // 4
    freq = ROPE_BASE ** (-np.arange(quarter, dtype=np.float64) / quarter)

    def table(positions, right):
        angle = np.asarray(positions, np.float64)[:, None] * freq[None, :]
        cos, sin = np.cos(angle), np.sin(angle)
        both = np.stack([np.concatenate([cos, cos], 1), np.concatenate([-sin, sin], 1)])
        blank = np.zeros_like(both)
        return np.concatenate([blank, both] if right else [both, blank], 2).astype(np.float32)

    rows = count // GRID_W
    return table(range(0, rows, 8), False), table(range(8), False), table(range(GRID_W), True)


def rms(v):
    return v * lax.rsqrt(jnp.mean(v * v, axis=-1, keepdims=True) + NORM_EPS)


def columns_of(mod, row, first, last):
    wide = mod.shape[2]
    found = []
    for piece in range(8):
        lo, hi = max(first - piece * wide, 0), min(last - piece * wide, wide)
        if lo < hi:
            found.append(tree([mod[8 * x + piece, row : row + 1, lo:hi] for x in range(4)], jnp.add))
    return jnp.concatenate(found, axis=1)


def tp_of(offset, core):
    return lax.rem(lax.axis_index("y") + offset + 4, 4) * 2 + core


def project_kernel(*refs):
    blocks, mod, far = list(refs[:7]), refs[7], refs[8:18]
    q_out, kv_out, buf = refs[18:21]
    held, arrived = refs[21:31], refs[31]
    copies = [pltpu.make_async_copy(f, h, arrived.at[i]) for i, (f, h) in enumerate(zip(far, held))]
    for copy in copies:
        copy.start()
    lat, wq, wk, wv, ctx, qg, kg, eights, ones, cols = held
    blocks.insert(0, lat)
    width = ctx.shape[1]
    rows = GRID_W
    sp = lax.axis_index("z") * 4 + lax.axis_index("x")
    core = lax.axis_index("c")

    vectors = [(columns_of(mod, r, width, 2 * width), columns_of(mod, r, 0, width)) for r in range(2)]

    def modulate(v, r):
        scale, offset = vectors[r]
        return (rms(v.astype(F32)) * (1.0 + scale) + offset).astype(BF)

    def turn(v, cos, sin):
        lane = lax.broadcasted_iota(jnp.int32, v.shape, 1)
        other = jnp.where(lane % 64 < 32, pltpu.roll(v, HD - 32, 1), pltpu.roll(v, 32, 1))
        return v * cos + other * sin

    def dot(a, b):
        return jnp.dot(a, b, preferred_element_type=F32)

    for side in range(2):
        for j in (1, 2, 3, 0) if side == 0 else range(4):
            if side == 0 and j == 0:
                for copy in copies:
                    copy.wait()
            buf[j * rows : (j + 1) * rows] = modulate(blocks[side * 4 + j][...], 0)
        normed = buf[...]
        q = dot(normed, wq[...])
        k = dot(normed, wk[...])
        v = dot(normed, wv[...]).astype(BF)
        k = rms(k) * kg[...]
        q0 = rms(q[:, :HD]) * qg[...]
        q1 = rms(q[:, HD:]) * qg[...]
        for j in range(4):
            at = slice(j * rows, (j + 1) * rows)
            tp = tp_of(OFFS[j], core if side == 0 else 1 - core)
            c8, s8, c1, s1 = (t[i, pl.ds(p, 1), :] for t, p in ((eights, sp), (ones, tp)) for i in (0, 1))
            cos = c8 * c1 - s8 * s1 + cols[0]
            sin = s8 * c1 + c8 * s1 + cols[1]
            to = pl.ds(pl.multiple_of(tp * rows, rows), rows)
            q_out[0, to, :] = turn(q0[at], cos, sin).astype(BF)
            q_out[1, to, :] = turn(q1[at], cos, sin).astype(BF)
            kv_out[to, :HD] = turn(k[at], cos, sin).astype(BF)
            kv_out[to, HD:] = v[at]
    normed = modulate(ctx[...], 1)
    total = 8 * rows
    kv_out[total:, :HD] = (rms(dot(normed, wk[...])) * kg[...]).astype(BF)
    kv_out[total:, HD:] = dot(normed, wv[...]).astype(BF)


def scores_of(q, keys):
    return lax.dot_general(q, keys, (((1,), (1,)), ((), ())), preferred_element_type=F32)


def tree(values, op):
    while len(values) > 1:
        odd = values[len(values) // 2 * 2 :]
        values = [op(values[2 * i], values[2 * i + 1]) for i in range(len(values) // 2)] + odd
    return values[0]


SCALE = HD**-0.5
C2 = SCALE * math.log2(math.e)
CHUNK = 512


def fill(k_buf, v_buf, pieces):
    for i, r in enumerate(pieces):
        at = slice(i * CHUNK, (i + 1) * CHUNK)
        k_buf[at] = r[:CHUNK, :HD]
        v_buf[at] = r[:CHUNK, HD:]


def softmax_block(q, k_buf, v_buf, before, lift=None):
    s = scores_of(q, k_buf[...])
    tiles = [s[:, i * HD : (i + 1) * HD] for i in range(s.shape[1] // HD)]
    if lift is not None:
        tiles = tiles[:-2] + [tiles[-2] + lift / SCALE]
    if before is None:
        blank = jnp.zeros((s.shape[0], HD), F32)
        before = (blank - 1e30, blank, blank)
    m_old, l_old, acc_old = before
    m_new = jnp.maximum(m_old, jnp.max(tree(tiles, jnp.maximum), axis=1, keepdims=True))
    base = m_new * C2
    alpha = jnp.exp2((m_old - m_new) * C2)
    probs = [jnp.exp2(t * C2 - base) for t in tiles]
    p = [t.astype(BF) for t in probs]
    if lift is not None:
        p.append(jnp.zeros((s.shape[0], HD), BF))
    pv = jnp.dot(jnp.concatenate(p, axis=1), v_buf[...], preferred_element_type=F32)
    return m_new, l_old * alpha + tree(probs, jnp.add), acc_old * alpha + pv


def rows_at(b, size=CHUNK):
    return pl.ds(pl.multiple_of(b * size, size), size)


def first_kernel(q, *refs):
    pieces, (m, l, acc, k_buf, v_buf) = refs[:-5], refs[-5:]
    fill(k_buf, v_buf, pieces)

    def step(b, carry):
        at, size = rows_at(b, CHUNK // 2), CHUNK // 2
        m[at], l[at], acc[at] = softmax_block(q[b // 2, rows_at(lax.rem(b, 2), size)], k_buf, v_buf, None)
        return carry

    lax.fori_loop(0, 4, step, 0)


def near_kernel(q0, q1, q2, m_own, l_own, acc_own, kv, up, down, q_all, m, l, acc, k_buf, v_buf):
    fill(k_buf, v_buf, (kv, up, down))
    for j, r in enumerate((q0, q1, q2)):
        for h in range(2):
            q_all[(2 * j + h) * CHUNK : (2 * j + h + 1) * CHUNK] = r[h]
    for whole, own in ((m, m_own), (l, l_own), (acc, acc_own)):
        whole[: 2 * CHUNK] = own[...]

    def step(b, carry):
        at = rows_at(b)
        m[at], l[at], acc[at] = softmax_block(q_all[at], k_buf, v_buf, None)
        return carry

    lax.fori_loop(2, 6, step, 0)


def more_kernel(q_all, m_in, l_in, acc_in, up, down, m, l, acc, k_buf, v_buf):
    fill(k_buf, v_buf, (up, down))

    def step(b, carry):
        at = rows_at(b)
        m[at], l[at], acc[at] = softmax_block(q_all[at], k_buf, v_buf, (m_in[at], l_in[at], acc_in[at]))
        return carry

    lax.fori_loop(0, q_all.shape[0] // CHUNK, step, 0)


def final_kernel(*refs, parts, lift, size):
    q_all, m_in, l_in, acc_in, up, down, opposite = refs[:7]
    tails = refs[7:14]
    outs, (k_buf, v_buf) = refs[14:-2], refs[-2:]
    fill(k_buf, v_buf, (up, down, opposite))
    at = 3 * CHUNK - 16
    for t in (opposite, *tails):
        at += 16
        k_buf[at : at + 16] = t[CHUNK:, :HD]
        v_buf[at : at + 16] = t[CHUNK:, HD:]
    at += 16
    k_buf[at:] = jnp.zeros((HD, HD), BF)
    v_buf[at:] = jnp.zeros((HD, HD), BF)

    subs = CHUNK // size

    def step(b, carry):
        at = rows_at(parts[0] * 2 * subs + b, size)
        sub, h = lax.rem(b, subs), lax.rem(b // subs, 2)
        m, l, acc = softmax_block(q_all[at], k_buf, v_buf, (m_in[at], l_in[at], acc_in[at]), lift)
        l = jnp.broadcast_to(jnp.sum(l, axis=1, keepdims=True), l.shape)
        values = (acc / l).astype(BF)
        lse = m * C2 + jnp.log2(l)
        packed = jnp.zeros((16, HD), F32)
        line = lax.broadcasted_iota(jnp.int32, (16, HD), 0)
        for t in range(size // HD):
            whole = lse[t * HD : (t + 1) * HD].T[:16]
            high = whole.astype(BF).astype(F32)
            mid = (whole - high).astype(BF).astype(F32)
            for i, v in enumerate((high, mid, whole - high - mid)):
                packed = jnp.where(line == 3 * (t + sub * (size // HD)) + i, v, packed)
        for i, out in enumerate(outs):

            @pl.when(b // (2 * subs) == i)
            def _(out=out):
                out[h, rows_at(sub, size)] = values
                rest = out[h, CHUNK:].astype(F32)
                out[h, CHUNK:] = jnp.where(
                    line < 3 * sub * (size // HD), rest, packed
                ).astype(BF)

        return carry

    lax.fori_loop(0, 2 * subs * len(parts), step, 0)


def merge_kernel(p0, p1, p2, p3, out):
    per = HD // GRID_W
    for h in range(2):
        tails = [p[h, CHUNK:].astype(F32) for p in (p0, p1, p2, p3)]
        for t in range(CHUNK // HD):
            lse = [v[3 * t : 3 * t + 1] + v[3 * t + 1 : 3 * t + 2] + v[3 * t + 2 : 3 * t + 3] for v in tails]
            top = tree(lse, jnp.maximum)
            share = [jnp.exp2(v - top) for v in lse]
            inv = 1.0 / tree(share, jnp.add)
            total = None
            for p, v in zip((p0, p1, p2, p3), share):
                w = jnp.broadcast_to(v * inv, (HD, HD)).T
                term = p[h, t * HD : (t + 1) * HD].astype(F32) * w
                total = term if total is None else total + term
            total = total.astype(BF)
            for i in range(per):
                out[t * per + i, :, h * HD : (h + 1) * HD] = total[i * GRID_W : (i + 1) * GRID_W]


def near(v):
    return pltpu.with_memory_space_constraint(v, pltpu.VMEM)


VMEM = pl.BlockSpec(memory_space=pltpu.VMEM)


def share_kernel(*refs):
    far, out, held, arrived = refs[:3], refs[3], refs[4:7], refs[7]
    copies = [pltpu.make_async_copy(f, h, arrived.at[i]) for i, (f, h) in enumerate(zip(far, held))]
    for copy in copies:
        copy.start()
    for copy in copies:
        copy.wait()
    both = jnp.concatenate([held[0][...], held[1][...]], axis=0)
    share = jnp.dot(
        jax.nn.silu(both), held[2][...], precision=lax.Precision.HIGHEST, preferred_element_type=F32
    )
    for i in range(out.shape[0]):
        out[i] = share


def call(kernel, operands, shape, keys, rows, alias=None):
    scratch = [pltpu.VMEM((keys, HD), BF)] * 2 if keys else []
    return pl.pallas_call(
        kernel,
        out_shape=shape,
        in_specs=[VMEM] * len(operands),
        out_specs=[VMEM] * len(shape),
        input_output_aliases=alias or {},
        scratch_shapes=scratch,
        compiler_params=pltpu.CompilerParams(vmem_limit_bytes=20 * 2**20),
        cost_estimate=pl.CostEstimate(
            flops=rows * max(keys, 128) * 4 * HD, transcendentals=rows * keys, bytes_accessed=2**20
        ),
    )(*[near(v) for v in operands])


def finish_kernel(got, w0, w1, w2, w3, w4, w5, w6, w7, lat, mod, out):
    core = lax.axis_index("c")
    width = lat.shape[1]
    mixed = None
    for j, weight in enumerate((w0, w1, w2, w3, w4, w5, w6, w7)):
        side, piece = j // 4, j % 4
        owner = core if side == 0 else 1 - core
        ahead = 1 - 2 * owner
        tp = tp_of((0, -ahead, ahead, 2)[piece], owner)
        part = jnp.dot(got[tp], weight[...], preferred_element_type=F32)
        mixed = part if mixed is None else mixed + part
    gate = columns_of(mod, 0, 2 * width, 3 * width)
    out[...] = (lat[...].astype(F32) + gate * rms(mixed)).astype(BF)


def body(
    latents, context, cond, ctx_cond, mod_weight, query_weight, key_matrix, value_matrix, out_weight,
    query_gain, key_gain,
):
    def over_four(v, axis):
        return [
            v,
            lax.ppermute(v, axis, shift(4, 1)),
            lax.ppermute(v, axis, shift(4, -1)),
            lax.ppermute(v, axis, shift(4, 2)),
        ]

    def swap(v):
        return lax.ppermute(v, "c", [(0, 1), (1, 0)])

    ahead = [(2 * i + c, 2 * ((i + 1 - 2 * c) % 4) + c) for i in range(4) for c in range(2)]
    behind = [(b, a) for a, b in ahead]

    mine = over_four(latents, "y")
    loaded = [cond[None], ctx_cond[None], mod_weight]
    shares = pl.pallas_call(
        share_kernel,
        out_shape=jax.ShapeDtypeStruct((16, 2, mod_weight.shape[1]), F32),
        in_specs=[pl.BlockSpec(memory_space=pltpu.HBM)] * 3,
        out_specs=VMEM,
        scratch_shapes=[pltpu.VMEM(v.shape, F32) for v in loaded] + [pltpu.SemaphoreType.DMA((3,))],
        name="share",
    )(*[pltpu.with_memory_space_constraint(v, pltpu.HBM) for v in loaded])
    shares = lax.all_to_all(shares, ("z", "c"), 0, 0)
    theirs = [swap(v) for v in mine]
    summed = jnp.sum(shares.reshape((8, 2) + shares.shape[1:]), axis=0)
    pieces = lax.all_to_all(jnp.broadcast_to(summed[None], (16,) + summed.shape), ("x", "y"), 0, 0)
    modulation = pieces.reshape((32,) + shares.shape[1:])
    count = 16384
    tables = [jnp.asarray(t) for t in rope_tables(count)]
    loaded = [
        latents, query_weight, key_matrix, value_matrix, context, query_gain[None], key_gain[None], *tables,
    ]
    q, kv = pl.pallas_call(
        project_kernel,
        out_shape=[pltpu.VMEM((2, 512, HD), BF), pltpu.VMEM((528, 2 * HD), BF)],
        in_specs=[VMEM] * 8 + [pl.BlockSpec(memory_space=pltpu.HBM)] * len(loaded),
        out_specs=[VMEM] * 2,
        scratch_shapes=[pltpu.VMEM((256, 2048), BF)]
        + [pltpu.VMEM(v.shape, v.dtype) for v in loaded]
        + [pltpu.SemaphoreType.DMA((len(loaded),))],
        compiler_params=pltpu.CompilerParams(vmem_limit_bytes=20 * 2**20),
        cost_estimate=pl.CostEstimate(flops=2 * 528 * 2048 * 512, transcendentals=0, bytes_accessed=4 * 2**20),
        name="project",
    )(
        *[near(v) for v in mine[1:] + theirs],
        near(modulation),
        *[pltpu.with_memory_space_constraint(v, pltpu.HBM) for v in loaded],
    )
    lift = math.log(count / (2.0 * 512))
    up, down = [kv], [kv]
    up.append(lax.ppermute(kv, "z", shift(8, 1)))
    down.append(lax.ppermute(kv, "z", shift(8, -1)))
    q_parts = over_four(q, "x")
    for _ in range(2):
        up.append(lax.ppermute(up[-1], "z", shift(8, 1)))
        down.append(lax.ppermute(down[-1], "z", shift(8, -1)))
    opposite = lax.ppermute(up[3], "z", shift(8, 1))
    first = lax.ppermute(out_weight, TP, ahead)
    second = lax.ppermute(out_weight, TP, behind)
    weights = [out_weight, first, second, lax.ppermute(out_weight, "y", shift(4, 2))]
    weights += [swap(v) for v in weights]

    state_of = lambda n: [pltpu.VMEM((n, HD), F32)] * 3
    firsts = [kv, up[1], down[1]]
    own = call(first_kernel, [q, *firsts], state_of(2 * CHUNK), 3 * CHUNK, 2 * CHUNK)
    q_all, *state = call(
        near_kernel, [*q_parts[:3], *own, *firsts],
        [pltpu.VMEM((6 * CHUNK, HD), BF)] + state_of(6 * CHUNK), 3 * CHUNK, 4 * CHUNK,
    )
    state = call(
        more_kernel, [q_all, *state, up[2], down[2]], state_of(6 * CHUNK), 2 * CHUNK, 6 * CHUNK,
        {1: 0, 2: 1, 3: 2},
    )
    far = call(first_kernel, [q_parts[3], *firsts, up[2], down[2]], state_of(2 * CHUNK), 5 * CHUNK, 2 * CHUNK)

    def final(whose, size, *parts):
        return call(
            functools.partial(final_kernel, parts=parts, lift=lift, size=size),
            [*whose, up[3], down[3], opposite, kv, *up[1:], *down[1:]],
            [pltpu.VMEM((2, CHUNK + 16, HD), BF)] * len(parts), 3 * CHUNK + 2 * HD, 2 * CHUNK * len(parts),
        )

    (to_far,) = final([q_parts[3].reshape(2 * CHUNK, HD), *far], CHUNK, 0)
    partials = [lax.ppermute(to_far, "x", shift(4, 2))]
    to_down, to_up = final([q_all, *state], CHUNK, 1, 2)
    partials.append(lax.ppermute(to_down, "x", shift(4, -1)))
    partials.append(lax.ppermute(to_up, "x", shift(4, 1)))
    partials += final([q_all, *state], CHUNK // 2, 0)
    (sent,) = call(merge_kernel, partials, [jax.ShapeDtypeStruct((8, GRID_W, 2 * HD), BF)], 0, CHUNK)
    got = lax.all_to_all(sent, TP, 0, 0)
    operands = [got, *weights, latents, modulation]
    return pl.pallas_call(
        finish_kernel,
        out_shape=jax.ShapeDtypeStruct(latents.shape, BF),
        in_specs=[VMEM] * len(operands),
        out_specs=VMEM,
        compiler_params=pltpu.CompilerParams(vmem_limit_bytes=20 * 2**20),
        cost_estimate=pl.CostEstimate(flops=2 * 64 * 2048 * 2048, transcendentals=0, bytes_accessed=10 * 2**20),
        name="finish",
    )(*[near(v) for v in operands])


def solution(mesh):
    torus = Mesh(mesh.devices.reshape(8, 4, 4, 2), ALL)
    placed = (
        P(ALL, None), P(SP, None), P(SP), P(SP), P(SP, TP), P(None, TP), P(None, TP), P(None, TP),
        P(TP, None), P(), P(),
    )

    return jax.shard_map(body, mesh=torus, in_specs=placed, out_specs=P(ALL, None), check_vma=False)
```
